32 devices in a mesh: grp: 2 (over y), sp: 4 (over z), tp: 4 (over x, core).
Axes of the slice: x: 2, y: 2, z: 4, core: 2. Of those that a mesh axis runs over, the one named last changes fastest.
Arguments:
- stream: bfloat16 [1024, 2048], P(('grp', 'sp')), parts along dimension 0, may hold values from -40 to 40
- queries: bfloat16 [1024, 1024], P(('grp', 'sp'), 'tp'), parts along dimension 0, may hold values from -6 to 6
- key_matrix: bfloat16 [1024, 1024], P(('grp', 'sp'), 'tp'), parts along dimension 0, may hold values from -6 to 6
- value_matrix: bfloat16 [1024, 2048], P(('grp', 'sp'), 'tp'), parts along dimension 0, may hold values from -6 to 6
- output_gate_logits: bfloat16 [1024, 2048], P(('grp', 'sp'), 'tp'), parts along dimension 0, may hold values from -6 to 6
- forgetting_raw_score: float32 [1024, 1024], P(('grp', 'sp'), 'tp'), parts along dimension 0, may hold values from -2 to 12
- additional_forgetting_rate: float32 [1024, 1024], P(('grp', 'sp'), 'tp'), parts along dimension 0, may hold values from -0.7 to 0
- head_norm_gain: float32 [2048], P('tp'), may hold values from 0.1 to 1.9
- output_weight: bfloat16 [2048, 2048], P('tp'), may hold values from -0.125 to 0.125
- feedforward_norm_gain: bfloat16 [2048], replicated, may hold values from 0.099609375 to 1.8984375
- gate_weight: bfloat16 [2048, 5632], P('sp', 'tp'), may hold values from -0.125 to 0.125
- up_weight: bfloat16 [2048, 5632], P('sp', 'tp'), may hold values from -0.125 to 0.125
- down_weight: bfloat16 [5632, 2048], P('tp', 'sp'), may hold values from -0.078125 to 0.078125
Outputs:
- layer_out: bfloat16 [1024, 2048], P(('grp', 'sp'), 'tp'), parts along dimension 0
The draws below stay inside these ranges and needn't reach their ends.
There are 2 independent parts, one for each index of `grp`. The reference program is written for one: setup_inputs(seed, part) draws one part's arguments, and reference() takes and returns one part's arrays. A program takes and returns all parts, laid end to end along the dimension named above; an argument that names none is the same for every part. Nothing has to cross between parts.
All inputs are finite; a program needn't handle non-finite values.
Results may differ from the reference program's by a relative error of at most 0.013.
Values may be sent and summed in bfloat16 or wider, within the bound.
A program may use at most 128 MiB of HBM per device.

```python
import math
import jax
import jax.numpy as jnp
from jax import lax

D = 2048
HEADS = 4
HK = 256
HV = 512
FF = 5632
BLOCK = 64
TOK_DEV = 128
SEQ = 512
KEYW = 1024
VALW = 2048
N_TP = 4


def draw_stream(key, part):
    first, second, third = jax.random.split(key, 3)
    noise = jnp.clip(jax.random.normal(first, (SEQ, D), jnp.float32), -4.0, 4.0)
    trend = jnp.arange(D, dtype=jnp.float32) / max(D - 1, 1)
    column_scale = jnp.exp(math.log(10.0) * (0.5 * trend + 0.5 * jax.random.uniform(second, (D,), jnp.float32)))
    row_scale = jnp.exp(jax.random.uniform(third, (SEQ, 1), jnp.float32, math.log(0.5), math.log(2.0)))
    return (noise * column_scale[None, :] * row_scale / 3.0).astype(jnp.bfloat16)


def draw_forgetting_raw_score(key, part):
    flag_key, slow_key, fast_key, device_key, noise_key = jax.random.split(key, 5)
    slow_flag = jax.random.randint(flag_key, (KEYW,), 0, 10) < 5
    sluggish_speed = jnp.exp(jax.random.uniform(slow_key, (KEYW,), jnp.float32, math.log(0.1), math.log(0.4))) / SEQ
    fast_rate = jnp.exp(jax.random.uniform(fast_key, (KEYW,), jnp.float32, math.log(0.01), math.log(1.0 / 30.0)))
    base_rate = jnp.where(slow_flag, sluggish_speed, fast_rate)
    device_factor = jnp.exp(jax.random.uniform(device_key, (SEQ // TOK_DEV, 1), jnp.float32, math.log(0.5), math.log(2.0)))
    device_factor = jnp.repeat(device_factor, TOK_DEV, axis=0)
    noise = jnp.exp(jax.random.uniform(noise_key, (SEQ, KEYW), jnp.float32, -0.5, 0.5))
    scaled = -16.0 * base_rate[None, :] * device_factor * noise
    logit = scaled - jnp.log(-jnp.expm1(scaled))
    return jnp.clip(logit, -2.0, 12.0)


def draw_additional_forgetting_rate(key, part):
    spot_key, depth_key = jax.random.split(key, 2)
    spots = jax.random.randint(spot_key, (3,), 0, SEQ)
    marked = jnp.any(jnp.arange(SEQ)[:, None] == spots[None, :], axis=1)
    depth = jax.random.uniform(depth_key, (SEQ, KEYW), jnp.float32, math.log(0.5), math.log(0.8))
    return jnp.where(marked[:, None], depth, 0.0)


def level_of(rng, extent, shards, low, top_value):
    def one(position, blocks):
        draws = jax.random.uniform(jax.random.fold_in(jax.random.fold_in(rng, 6), position), (blocks,), jnp.float32, low / len(shards), top_value / len(shards))
        return jnp.repeat(jnp.exp(draws), extent[position] // blocks).reshape((-1,) + (1,) * (len(extent) - position - 1))

    loudness = one(*shards[0])
    for cut in shards[1:]:
        loudness = loudness * one(*cut)
    return loudness


def scatter_about(own_key, extent, scale, limit, shards=(), kind=jnp.bfloat16):
    array = jax.random.normal(own_key, extent, jnp.float32) * scale
    if len(shards) > 0:
        array = level_of(own_key, extent, shards, -0.22, 0.18) * array
    return jnp.clip(array, min=-limit, max=limit).astype(kind)


def setup_inputs(seed: int = 0, part: int = 0) -> dict:
    splits = jax.random.split(jax.random.key(seed), 14)
    own_keys = jax.random.split(jax.random.fold_in(splits[13], part), 14)
    return {
        "stream": draw_stream(jax.random.fold_in(jax.random.fold_in(splits[13], part), 71), part),
        "queries": scatter_about(own_keys[1], (SEQ, KEYW), 1.0, 6.0, ((0, 4), (1, 4))),
        "key_matrix": scatter_about(own_keys[2], (SEQ, KEYW), 1.0, 6.0, ((0, 4), (1, 4))),
        "value_matrix": scatter_about(own_keys[3], (SEQ, VALW), 1.0, 6.0, ((0, 4), (1, 4))),
        "output_gate_logits": scatter_about(own_keys[4], (SEQ, VALW), 1.0, 6.0, ((0, 4), (1, 4))),
        "forgetting_raw_score": draw_forgetting_raw_score(jax.random.fold_in(jax.random.fold_in(splits[13], part), 71), part),
        "additional_forgetting_rate": draw_additional_forgetting_rate(jax.random.fold_in(jax.random.fold_in(splits[13], part), 71), part),
        "head_norm_gain": jnp.clip(1.0 + 0.18 * jax.random.normal(splits[7], (VALW,), jnp.float32), 0.1, 1.9),
        "output_weight": scatter_about(splits[8], (VALW, D), VALW ** -0.5, 0.125, ((0, 4),)),
        "feedforward_norm_gain": jnp.clip(1.0 + 0.18 * jax.random.normal(splits[9], (D,), jnp.float32), 0.099609375, 1.8984375).astype(jnp.bfloat16),
        "gate_weight": scatter_about(splits[10], (D, FF), D ** -0.5, 0.125, ((0, 4), (1, 4))),
        "up_weight": scatter_about(splits[11], (D, FF), D ** -0.5, 0.125, ((0, 4), (1, 4))),
        "down_weight": scatter_about(splits[12], (FF, D), FF ** -0.5, 0.078125, ((0, 4), (1, 4))),
    }


epsilon = 1e-06
sigmoid_sharpness = 16.0
highest = lax.Precision.HIGHEST

def split_heads(tensor, blocks, depth):
    return tensor.astype(jnp.float32).reshape(blocks, BLOCK, HEADS, depth).transpose(2, 0, 1, 3)

def block_attention(queries, key_matrix, value_matrix, forgetting_exponent):
    blocks = SEQ // BLOCK
    query_part = split_heads(queries, blocks, HK) * HK ** (-0.5)
    key_part = split_heads(key_matrix, blocks, HK)
    value_part = split_heads(value_matrix, blocks, HV)
    decay_part = split_heads(forgetting_exponent, blocks, HK)
    within = jnp.cumsum(decay_part, axis=2)
    closing = within[:, :, -1, :]
    query_in = query_part * jnp.exp(within)
    key_in = key_part * jnp.exp(-within)
    key_end = key_part * jnp.exp(closing[:, :, None, :] - within)
    causal = jnp.tril(jnp.ones((BLOCK, BLOCK), jnp.bool_))
    scores = jnp.einsum('hntd,hnsd->hnts', query_in, key_in, precision=highest)
    scores = jnp.where(causal, scores, 0.0)
    inside = jnp.einsum('hnts,hnsv->hntv', scores, value_part, precision=highest)

    def advance(memory, inputs):
        query_block, key_block, value_block, decay_block = inputs
        final_answer = jnp.einsum('htd,hdv->htv', query_block, memory, precision=highest)
        memory = decay_block[:, :, None] * memory + jnp.einsum('hsd,hsv->hdv', key_block, value_block, precision=highest)
        return (memory, final_answer)
    sequence = (jnp.moveaxis(query_in, 1, 0), jnp.moveaxis(key_end, 1, 0), jnp.moveaxis(value_part, 1, 0), jnp.moveaxis(jnp.exp(closing), 1, 0))
    start_memory = jnp.zeros((HEADS, HK, HV), jnp.float32)
    _, earlier_blocks = lax.scan(advance, start_memory, sequence)
    combined = inside + jnp.moveaxis(earlier_blocks, 0, 1)
    return combined.transpose(1, 2, 0, 3).reshape(SEQ, HEADS, HV)

def group_sum(left, weight):
    share = weight.shape[0] // N_TP
    totals = jnp.zeros((left.shape[0], weight.shape[1]), jnp.float32)
    for group in range(N_TP):
        product = jnp.dot(left[:, group * share:(group + 1) * share], weight[group * share:(group + 1) * share], preferred_element_type=jnp.float32)
        rounded = lax.optimization_barrier(product.astype(jnp.bfloat16))
        totals = totals + rounded.astype(jnp.float32)
    return totals

def reference(stream, queries, key_matrix, value_matrix, output_gate_logits, forgetting_raw_score, additional_forgetting_rate, head_norm_gain, output_weight, feedforward_norm_gain, gate_weight, up_weight, down_weight):
    forgetting_exponent = jax.nn.log_sigmoid(forgetting_raw_score) / sigmoid_sharpness + additional_forgetting_rate
    attn_heads = block_attention(queries, key_matrix, value_matrix, forgetting_exponent)
    attn_heads = attn_heads * lax.rsqrt(lax.optimization_barrier(jnp.mean(attn_heads * attn_heads, axis=-1, keepdims=True)) + epsilon)
    gated_rows = (attn_heads.reshape(SEQ, VALW) * head_norm_gain * jax.nn.silu(output_gate_logits.astype(jnp.float32))).astype(jnp.bfloat16)
    attn_out = group_sum(gated_rows, output_weight)
    resid = stream.astype(jnp.float32) + attn_out
    normed = (resid * lax.rsqrt(lax.optimization_barrier(jnp.mean(resid * resid, axis=-1, keepdims=True)) + epsilon) * feedforward_norm_gain.astype(jnp.float32)).astype(jnp.bfloat16)
    gate_sum = jnp.dot(normed, gate_weight, preferred_element_type=jnp.float32)
    up_sum = jnp.dot(normed, up_weight, preferred_element_type=jnp.float32)
    hidden = (jax.nn.silu(gate_sum) * up_sum).astype(jnp.bfloat16)
    ffn_out = group_sum(hidden, down_weight)
    return (resid + ffn_out).astype(jnp.bfloat16)
```

```python
import jax
import jax.numpy as jnp
from jax import lax
from jax.sharding import PartitionSpec as P

HK = 256
HV = 512
BLOCK = 64


epsilon = 1e-06
sigmoid_sharpness = 16.0
highest = lax.Precision.HIGHEST


def carried_in(value, axis, join, neutral):
    place = lax.axis_index(axis)
    gathered = jax.tree.map(
        lambda a, kind: lax.all_gather(a.astype(kind), axis), value, (jnp.bfloat16, jnp.bfloat16)
    )
    state = jax.tree.map(lambda a, e: jnp.zeros_like(a) + jnp.asarray(e, a.dtype), value, neutral)

    def one(turn, state):
        return join(
            state,
            jax.tree.map(
                lambda a, own: lax.dynamic_index_in_dim(a, turn, 0, False).astype(own.dtype),
                gathered,
                value,
            ),
        )

    return lax.fori_loop(0, place, one, state)


def split_heads(tensor, blocks, count, depth):
    return tensor.astype(jnp.float32).reshape(blocks, BLOCK, count, depth).transpose(2, 0, 1, 3)


def combine(earlier, later):
    return (earlier[0] * later[0], later[0][:, :, None] * earlier[1] + later[1])


def swap_units(weight, unit_axis):
    places = lax.axis_size("sp")
    copies = lax.axis_size("grp")
    place = lax.axis_index("sp")
    copy = lax.axis_index("grp")
    other = 1 - unit_axis
    units = weight.shape[unit_axis] // places
    depth = weight.shape[other]
    part = depth // copies
    shape = [0, 0]
    shape[unit_axis] = units
    shape[other] = depth * places
    whole = jnp.zeros(shape, weight.dtype)

    def put(whole, block, at):
        return lax.dynamic_update_slice_in_dim(whole, block, at, other)

    own = lax.dynamic_slice_in_dim(weight, place * units, units, unit_axis)
    pieces = []
    for shift in range(1, places):
        target = (place + shift) % places
        block = lax.dynamic_slice_in_dim(weight, target * units, units, unit_axis)
        block = lax.dynamic_slice_in_dim(block, copy * part, part, other)
        ring = [(i, (i + shift) % places) for i in range(places)]
        pieces.append((shift, lax.ppermute(block, "sp", ring)))
    whole = put(whole, own, place * depth)
    for shift, block in pieces:
        source = (place - shift) % places
        whole = put(whole, block, source * depth + copy * part)
        for turn in range(1, copies):
            ring = [(i, (i + turn) % copies) for i in range(copies)]
            passed = lax.ppermute(block, "grp", ring)
            whole = put(whole, passed, source * depth + ((copy - turn) % copies) * part)
    return whole


def spread_units(normed_part, gate_weight, up_weight, down_weight):
    normed = lax.all_gather(normed_part, ("sp", "tp"))
    places = lax.axis_size("sp")
    shares = lax.axis_size("tp")
    tokens, width = normed_part.shape
    normed = normed.reshape(places, shares, tokens, width).transpose(0, 2, 1, 3)
    normed = normed.reshape(places * tokens, shares * width)
    gate = swap_units(gate_weight, 1)
    up = swap_units(up_weight, 1)
    down = swap_units(down_weight, 0)
    gate_sum = jnp.dot(normed, gate, preferred_element_type=jnp.float32)
    up_sum = jnp.dot(normed, up, preferred_element_type=jnp.float32)
    hidden = (jax.nn.silu(gate_sum) * up_sum).astype(jnp.bfloat16)
    down_sum = jnp.dot(hidden, down, preferred_element_type=jnp.float32).astype(jnp.bfloat16)
    down_sum = lax.psum_scatter(down_sum, "sp", scatter_dimension=0, tiled=True)
    return lax.psum_scatter(down_sum, "tp", scatter_dimension=1, tiled=True)


def local(
    stream,
    queries,
    key_matrix,
    value_matrix,
    output_gate_logits,
    forgetting_raw_score,
    additional_forgetting_rate,
    head_norm_gain,
    output_weight,
    feedforward_norm_gain,
    gate_weight,
    up_weight,
    down_weight,
):
    tokens = queries.shape[0]
    owned_heads = queries.shape[1] // HK
    blocks = tokens // BLOCK
    forgetting_exponent = (
        jax.nn.log_sigmoid(forgetting_raw_score) / sigmoid_sharpness + additional_forgetting_rate
    )
    query_part = split_heads(queries, blocks, owned_heads, HK) * HK ** (-0.5)
    key_part = split_heads(key_matrix, blocks, owned_heads, HK)
    value_part = split_heads(value_matrix, blocks, owned_heads, HV)
    decay_part = split_heads(forgetting_exponent, blocks, owned_heads, HK)
    within = jnp.cumsum(decay_part, axis=2)
    closing = within[:, :, -1, :]
    query_in = query_part * jnp.exp(within)
    key_in = key_part * jnp.exp(-within)
    key_end = key_part * jnp.exp(closing[:, :, None, :] - within)
    causal = jnp.tril(jnp.ones((BLOCK, BLOCK), jnp.bool_))
    scores = jnp.einsum("hntd,hnsd->hnts", query_in, key_in, precision=highest)
    scores = jnp.where(causal, scores, 0.0)
    inside = jnp.einsum("hnts,hnsv->hntv", scores, value_part, precision=highest)

    def advance(memory, inputs):
        query_block, key_block, value_block, decay_block = inputs
        final_answer = jnp.einsum("htd,hdv->htv", query_block, memory, precision=highest)
        memory = decay_block[:, :, None] * memory + jnp.einsum(
            "hsd,hsv->hdv", key_block, value_block, precision=highest
        )
        return (memory, final_answer)

    sequence = (
        jnp.moveaxis(query_in, 1, 0),
        jnp.moveaxis(key_end, 1, 0),
        jnp.moveaxis(value_part, 1, 0),
        jnp.moveaxis(jnp.exp(closing), 1, 0),
    )
    start_memory = jnp.zeros((owned_heads, HK, HV), jnp.float32)
    final_memory, earlier_blocks = lax.scan(advance, start_memory, sequence)
    device_decay = jnp.exp(jnp.sum(closing, axis=1))
    neutral = (jnp.ones_like(device_decay), jnp.zeros_like(final_memory))
    _, carried = carried_in((device_decay, final_memory), "sp", combine, neutral)
    before = jnp.cumsum(closing, axis=1) - closing
    query_far = query_in * jnp.exp(before[:, :, None, :])
    outside = jnp.einsum("hntd,hdv->hntv", query_far, carried, precision=highest)
    mixed_heads = inside + jnp.moveaxis(earlier_blocks, 0, 1) + outside
    mixed_heads = mixed_heads.transpose(1, 2, 0, 3).reshape(tokens, owned_heads, HV)
    mixed_heads = mixed_heads * lax.rsqrt(
        jnp.mean(mixed_heads * mixed_heads, axis=-1, keepdims=True) + epsilon
    )
    gated_rows = (
        mixed_heads.reshape(tokens, owned_heads * HV)
        * head_norm_gain
        * jax.nn.silu(output_gate_logits.astype(jnp.float32))
    ).astype(jnp.bfloat16)
    partial_out = jnp.dot(gated_rows, output_weight, preferred_element_type=jnp.float32)
    model_width = stream.shape[1]
    column_share = model_width // lax.axis_size("tp")
    column_start = lax.axis_index("tp") * column_share
    attn_cols = lax.psum_scatter(
        partial_out.astype(jnp.bfloat16), "tp", scatter_dimension=1, tiled=True
    ).astype(jnp.float32)
    resid_part = (
        lax.dynamic_slice_in_dim(stream, column_start, column_share, 1).astype(jnp.float32)
        + attn_cols
    )
    elementwise_power = lax.psum(jnp.sum(resid_part * resid_part, axis=1), "tp")
    gain_part = lax.dynamic_slice_in_dim(
        feedforward_norm_gain, column_start, column_share, 0
    ).astype(jnp.float32)
    rescaled_portion = (
        resid_part * lax.rsqrt(elementwise_power / model_width + epsilon)[:, None] * gain_part
    ).astype(jnp.bfloat16)
    places = lax.axis_size("sp")
    hidden_share = gate_weight.shape[1]
    moved = 2 * tokens * places * model_width
    if moved < 3 * model_width * hidden_share and hidden_share % places == 0:
        down_sum = spread_units(rescaled_portion, gate_weight, up_weight, down_weight)
        ffn_part = down_sum.astype(jnp.float32)
        return (resid_part + ffn_part).astype(jnp.bfloat16)
    normed = lax.all_gather(rescaled_portion, "tp", axis=1, tiled=True)
    gate_sum = jnp.dot(
        normed,
        lax.all_gather(gate_weight, "sp", axis=0, tiled=True),
        preferred_element_type=jnp.float32,
    )
    up_sum = jnp.dot(
        normed,
        lax.all_gather(up_weight, "sp", axis=0, tiled=True),
        preferred_element_type=jnp.float32,
    )
    hidden = (jax.nn.silu(gate_sum) * up_sum).astype(jnp.bfloat16)
    down_sum = jnp.dot(
        hidden,
        lax.all_gather(down_weight, "sp", axis=1, tiled=True),
        preferred_element_type=jnp.float32,
    )
    ffn_part = lax.psum_scatter(
        down_sum.astype(jnp.bfloat16), "tp", scatter_dimension=1, tiled=True
    ).astype(jnp.float32)
    return (resid_part + ffn_part).astype(jnp.bfloat16)


def solution(mesh):
    return jax.shard_map(
        local,
        mesh=mesh,
        in_specs=(
            P(("grp", "sp"), None),
            P(("grp", "sp"), "tp"),
            P(("grp", "sp"), "tp"),
            P(("grp", "sp"), "tp"),
            P(("grp", "sp"), "tp"),
            P(("grp", "sp"), "tp"),
            P(("grp", "sp"), "tp"),
            P("tp"),
            P("tp", None),
            P(),
            P("sp", "tp"),
            P("sp", "tp"),
            P("tp", "sp"),
        ),
        out_specs=P(("grp", "sp"), "tp"),
        check_vma=False,
    )
```

```python
import functools
import jax
import jax.numpy as jnp
from jax import lax
from jax.sharding import PartitionSpec as P
from jax.experimental import pallas as pl
from jax.experimental.pallas import tpu as pltpu

HK = 256
HV = 512
BLOCK = 64


epsilon = 1e-06
sigmoid_sharpness = 16.0
highest = lax.Precision.HIGHEST


def carried_in(value, axis, join, neutral):
    place = lax.axis_index(axis)
    gathered = jax.tree.map(
        lambda a, kind: lax.all_gather(a.astype(kind), axis), value, (jnp.bfloat16, jnp.bfloat16)
    )
    state = jax.tree.map(lambda a, e: jnp.zeros_like(a) + jnp.asarray(e, a.dtype), value, neutral)

    def one(turn, state):
        return join(
            state,
            jax.tree.map(
                lambda a, own: lax.dynamic_index_in_dim(a, turn, 0, False).astype(own.dtype),
                gathered,
                value,
            ),
        )

    return lax.fori_loop(0, place, one, state)


def split_heads(tensor, blocks, count, depth):
    return tensor.astype(jnp.float32).reshape(blocks, BLOCK, count, depth).transpose(2, 0, 1, 3)


def combine(earlier, later):
    return (earlier[0] * later[0], later[0][:, :, None] * earlier[1] + later[1])


def nt_dot(a, b):
    return lax.dot_general(a, b, (((1,), (1,)), ((), ())), preferred_element_type=jnp.float32)


def fused_kernel(
    places, shares, copies, units,
    stream, queries, keys, values, out_gate, raw_score, extra_rate, head_gain, ffn_gain,
    out_weight, gate_weight, up_weight, down_weight,
    out,
    gate_buf, up_buf, down_buf, wo_buf, state_own, state_in, decay_own, decay_in, attn,
    proj_out, proj_in, resid, y_all, square_own, square_in, total,
    pair_out, pair_in, held, cross_out, cross_in, line_out, line_in,
    local_sem, wide_send, wide_recv, pass_send, pass_recv, state_send, state_recv,
    decay_send, decay_recv, proj_send, proj_recv, square_send, square_recv,
    total_send, total_recv, line_y_send, line_y_recv, core_send, core_recv,
    chip_send, chip_recv, relay_send, relay_recv, pair_send, pair_recv,
    cross_send, cross_recv, sum_send, sum_recv,
):
    s = lax.axis_index("sp")
    t = lax.axis_index("tp")
    g = lax.axis_index("grp")
    f32, bf16 = jnp.float32, jnp.bfloat16
    tokens = queries.shape[0]
    cols = out.shape[1]
    model_width = stream.shape[1]
    depth = gate_weight.shape[0]
    part = depth // copies
    excess = places * units - gate_weight.shape[1]
    blocks = tokens // BLOCK

    def send(src, dst, send_sem, recv_sem, **where):
        return pltpu.make_async_remote_copy(
            src_ref=src, dst_ref=dst, send_sem=send_sem, recv_sem=recv_sem,
            device_id=where, device_id_type=pl.DeviceIdType.MESH,
        )

    def up_by(k):
        return lax.rem(s + k, places)

    def down_by(k):
        return lax.rem(s + places - k, places)

    def offset(i):
        return pl.multiple_of(i * units - (i // (places - 1)) * excess, 128)

    weights = ((gate_weight, gate_buf), (up_weight, up_buf), (down_weight, down_buf))

    def region(m, source, copy, size):
        at = pl.ds(pl.multiple_of(source * depth + copy * part, 128), size)
        return weights[m][1].at[:, at] if m == 2 else weights[m][1].at[at, :]

    def source_of(m, target, copy, size):
        at = pl.ds(pl.multiple_of(copy * part, 128), size)
        chosen = pl.ds(offset(target), units)
        return weights[m][0].at[chosen, at] if m == 2 else weights[m][0].at[at, chosen]

    def wide(k, m):
        return send(
            source_of(m, up_by(k), g, part), region(m, s, g, part),
            wide_send.at[k - 1, m], wide_recv.at[k - 1, m], sp=up_by(k),
        )

    def passed(k, m, turn):
        here = region(m, down_by(k), g, part)
        return send(
            here, here, pass_send.at[turn - 1, k - 1, m], pass_recv.at[turn - 1, k - 1, m],
            grp=lax.rem(g + turn, copies),
        )

    own = [
        pltpu.make_async_copy(source_of(m, s, 0, depth), region(m, s, 0, depth), local_sem.at[m])
        for m in range(3)
    ]
    load_out = pltpu.make_async_copy(out_weight, wo_buf, local_sem.at[3])
    load_out.start()
    for copy in own:
        copy.start()

    barrier = pltpu.get_barrier_semaphore()
    for k in range(1, places):
        pl.semaphore_signal(barrier, inc=1, device_id={"sp": up_by(k)}, device_id_type=pl.DeviceIdType.MESH)
    for j in range(1, shares):
        pl.semaphore_signal(
            barrier, inc=1, device_id={"tp": lax.rem(t + j, shares)}, device_id_type=pl.DeviceIdType.MESH
        )
    for j in range(1, copies):
        pl.semaphore_signal(
            barrier, inc=1, device_id={"grp": lax.rem(g + j, copies)}, device_id_type=pl.DeviceIdType.MESH
        )
    pl.semaphore_wait(barrier, places + shares + copies - 3)

    wide(1, 0).start()

    score = raw_score[...]
    decay = (
        -(jnp.maximum(-score, 0.0) + jnp.log1p(jnp.exp(-jnp.abs(score)))) / sigmoid_sharpness
        + extra_rate[...]
    )
    row = lax.broadcasted_iota(jnp.int32, (tokens, tokens), 0)
    col = lax.broadcasted_iota(jnp.int32, (tokens, tokens), 1)
    causal = row >= col
    running = jnp.dot(
        jnp.where(causal, 1.0, 0.0), decay, precision=highest, preferred_element_type=f32
    )
    last = running[tokens - 1 : tokens, :]
    key = keys[...].astype(f32)
    value = values[...]
    key_end = (key * jnp.exp(last - running)).astype(bf16)
    state_own[...] = lax.dot_general(
        key_end, value, (((0,), (0,)), ((), ())), preferred_element_type=f32
    ).astype(bf16)
    decay_own[...] = jnp.broadcast_to(last, decay_own.shape)

    def state_copies(k):
        return (
            send(decay_own, decay_in.at[k - 1], decay_send.at[k - 1], decay_recv.at[k - 1], sp=up_by(k)),
            send(state_own, state_in.at[k - 1], state_send.at[k - 1], state_recv.at[k - 1], sp=up_by(k)),
        )

    for k in range(1, places):

        @pl.when(s + k < places)
        def _():
            for copy in state_copies(k):
                copy.start()

    for k in range(2, places):
        wide(k, 0).start()
    for k in range(1, places):
        wide(k, 1).start()

    query = queries[...].astype(f32) * HK ** (-0.5)
    pieces = []
    for b in range(blocks):
        rows = slice(b * BLOCK, (b + 1) * BLOCK)
        begin = jnp.zeros_like(last) if b == 0 else running[b * BLOCK - 1 : b * BLOCK, :]
        inner = running[rows] - begin
        scores = nt_dot(
            (query[rows] * jnp.exp(inner)).astype(bf16), (key[rows] * jnp.exp(-inner)).astype(bf16)
        )
        scores = jnp.where(causal[:BLOCK, :BLOCK], scores, 0.0).astype(bf16)
        piece = jnp.dot(scores, value[rows], preferred_element_type=f32)
        for c in range(b):
            old = slice(c * BLOCK, (c + 1) * BLOCK)
            close = running[(c + 1) * BLOCK - 1 : (c + 1) * BLOCK, :]
            far = nt_dot(
                (query[rows] * jnp.exp(running[rows] - close)).astype(bf16),
                (key[old] * jnp.exp(close - running[old])).astype(bf16),
            )
            piece = piece + jnp.dot(far.astype(bf16), value[old], preferred_element_type=f32)
        attn[rows, :] = piece

    logits = out_gate[...].astype(f32)
    gate_factor = head_gain[...] * (logits / (1.0 + jnp.exp(-logits)))
    query_far = query * jnp.exp(running)
    for k in range(1, places):

        @pl.when(s >= k)
        def _():
            for copy in state_copies(k):
                copy.wait_recv()
            between = jnp.zeros_like(last)
            for j in range(1, k):
                between = between + decay_in[j - 1, 0:1, :]
            attn[...] += jnp.dot(
                (query_far * jnp.exp(between)).astype(bf16), state_in[k - 1],
                preferred_element_type=f32,
            )

    heads = attn[...]
    heads = heads * lax.rsqrt(jnp.mean(heads * heads, axis=-1, keepdims=True) + epsilon)
    gated = (heads * gate_factor).astype(bf16)
    load_out.wait()

    def columns(i):
        return pl.ds(pl.multiple_of(i * cols, 128), cols)

    def proj_copy(j):
        target = lax.rem(t + j, shares)
        return send(
            proj_out.at[j], proj_in.at[j - 1], proj_send.at[j - 1], proj_recv.at[j - 1], tp=target
        )

    for j in (2, 3, 1, 0) if shares == 4 else range(shares - 1, -1, -1):
        target = lax.rem(t + j, shares)
        proj_out[j] = jnp.dot(gated, wo_buf[:, columns(target)], preferred_element_type=f32).astype(bf16)
        if j > 0:
            proj_copy(j).start()

    for k in range(1, places):
        wide(k, 0).wait_recv()
        for turn in range(1, copies):
            passed(k, 0, turn).start()

    joined = proj_out[0].astype(f32)
    for j in range(1, shares):
        proj_copy(j).wait_recv()
        joined = joined + proj_in[j - 1].astype(f32)
    joined = stream[:, columns(t)].astype(f32) + joined
    resid[...] = joined
    square_own[...] = lax.dot_general(
        jnp.ones((8, cols), f32), joined * joined, (((1,), (1,)), ((), ())),
        precision=highest, preferred_element_type=f32,
    )
    y_all[s, t] = (joined * ffn_gain[:, columns(t)].astype(f32)).astype(bf16)

    def square_copy(j):
        return send(
            square_own, square_in.at[j - 1], square_send.at[j - 1], square_recv.at[j - 1],
            tp=lax.rem(t + j, shares),
        )

    def total_copy(k):
        return send(total.at[0], total.at[k], total_send.at[k - 1], total_recv.at[k - 1], sp=up_by(k))

    def line_y(k):
        mine = y_all.at[s, t]
        return send(mine, mine, line_y_send.at[k - 1], line_y_recv.at[k - 1], sp=up_by(k))

    half = shares // 2
    near = t + 1 - 2 * lax.rem(t, 2)
    across = lax.rem(t + half, shares)
    diagonal = lax.rem(near + half, shares)

    def core_y(k):
        held_y = y_all.at[down_by(k), t]
        return send(held_y, held_y, core_send.at[k], core_recv.at[k], tp=near)

    def chip_y(k):
        held_y = y_all.at[down_by(k), t]
        return send(held_y, held_y, chip_send.at[k], chip_recv.at[k], tp=across)

    def relay_y(k):
        held_y = y_all.at[down_by(k), across]
        return send(held_y, held_y, relay_send.at[k], relay_recv.at[k], tp=near)

    for j in range(1, shares):
        square_copy(j).start()
    for k in range(1, places):
        line_y(k).start()
    chip_y(0).start()
    core_y(0).start()
    for k in range(1, places):
        wide(k, 2).start()
    squares = square_own[...]
    for j in range(1, shares):
        square_copy(j).wait_recv()
        squares = squares + square_in[j - 1]
    total[0] = squares
    for k in range(1, places):
        total_copy(k).start()
    for k in range(1, places):
        wide(k, 1).wait_recv()
        for turn in range(1, copies):
            passed(k, 1, turn).start()
    chip_y(0).wait_recv()
    relay_y(0).start()
    for k in range(1, places):
        line_y(k).wait_recv()
        chip_y(k).start()
        core_y(k).start()
    for k in range(1, places):
        chip_y(k).wait_recv()
        relay_y(k).start()
    for m in range(2):
        own[m].wait()
        for k in range(1, places):
            for turn in range(1, copies):
                passed(k, m, turn).wait_recv()
    own[2].wait()
    unit_at = lax.broadcasted_iota(jnp.int32, (tokens, units), 1)
    keep = unit_at >= (s // (places - 1)) * excess
    identity = jnp.where(row == col, 1.0, 0.0)

    def pair_copy(k):
        return send(pair_out.at[k], pair_in.at[k], pair_send.at[k], pair_recv.at[k], tp=near)

    def cross_copy(k):
        return send(cross_out.at[k], cross_in.at[k], cross_send.at[k], cross_recv.at[k], tp=across)

    def sum_copy(k):
        return send(line_out.at[k], line_in.at[k], sum_send.at[k], sum_recv.at[k], sp=down_by(k))

    def pair_step(k):
        pair_copy(k).wait_recv()
        cross_out[k] = (held[k, 1] + pair_in[k, 1].astype(f32)).astype(bf16)
        cross_copy(k).start()
        held[k, 0] = held[k, 0] + pair_in[k, 0].astype(f32)

    def cross_step(k):
        cross_copy(k).wait_recv()
        if k == 0:
            held[k, 0] = held[k, 0] + cross_in[k].astype(f32)
        else:
            line_out[k] = (held[k, 0] + cross_in[k].astype(f32)).astype(bf16)
            sum_copy(k).start()

    order = list(range(1, places)) + [0]
    for turn_at, k in enumerate(order):
        block = down_by(k)
        core_y(k).wait_recv()
        relay_y(k).wait_recv()
        if k > 0:
            total_copy(k).wait_recv()
        scale = lax.dot_general(
            identity, total[k], (((1,), (1,)), ((), ())), precision=highest, preferred_element_type=f32
        )[:, 0:1]
        scale = lax.rsqrt(scale / model_width + epsilon)
        gate_sum = jnp.zeros((tokens, units), f32)
        up_sum = jnp.zeros((tokens, units), f32)
        for i in range(shares):
            y = y_all[block, i]
            here = slice(i * cols, (i + 1) * cols)
            gate_sum = gate_sum + jnp.dot(y, gate_buf[here, :], preferred_element_type=f32)
            up_sum = up_sum + jnp.dot(y, up_buf[here, :], preferred_element_type=f32)
        gate_sum = gate_sum * scale
        up_sum = up_sum * scale
        hidden = gate_sum / (1.0 + jnp.exp(-gate_sum)) * up_sum
        hidden = jnp.where(keep, hidden, 0.0).astype(bf16)
        if turn_at == 0:
            for q in range(1, places):
                wide(q, 2).wait_recv()
                for turn in range(1, copies):
                    passed(q, 2, turn).start()
            for q in range(1, places):
                for turn in range(1, copies):
                    passed(q, 2, turn).wait_recv()
        for i, target in enumerate((near, diagonal)):
            pair_out[k, i] = jnp.dot(
                hidden, down_buf[:, columns(target)], preferred_element_type=f32
            ).astype(bf16)
        pair_copy(k).start()
        for i, target in enumerate((t, across)):
            held[k, i] = jnp.dot(hidden, down_buf[:, columns(target)], preferred_element_type=f32)
        if turn_at > 0:
            pair_step(order[turn_at - 1])
        if turn_at > 1:
            cross_step(order[turn_at - 2])
    pair_step(order[-1])
    for k in order[-2:]:
        cross_step(k)
    result = resid[...] + held[0, 0]
    for k in range(1, places):
        sum_copy(k).wait_recv()
        result = result + line_in[k].astype(f32)
    out[...] = result.astype(bf16)

    for k in range(1, places):

        @pl.when(s + k < places)
        def _():
            for copy in state_copies(k):
                copy.wait_send()

        for m in range(3):
            wide(k, m).wait_send()
            for turn in range(1, copies):
                passed(k, m, turn).wait_send()
        total_copy(k).wait_send()
        line_y(k).wait_send()
        sum_copy(k).wait_send()
    for j in range(1, shares):
        proj_copy(j).wait_send()
        square_copy(j).wait_send()
    for k in range(places):
        for copy in (core_y, chip_y, relay_y, pair_copy, cross_copy):
            copy(k).wait_send()


def fused(units, *arrays):
    (
        stream, queries, key_matrix, value_matrix, output_gate_logits, forgetting_raw_score,
        additional_forgetting_rate, head_norm_gain, output_weight, feedforward_norm_gain,
        gate_weight, up_weight, down_weight,
    ) = arrays
    places, shares, copies = (lax.axis_size(a) for a in ("sp", "tp", "grp"))
    tokens, model_width = stream.shape
    cols = model_width // shares
    f32, bf16 = jnp.float32, jnp.bfloat16
    vmem = pl.BlockSpec(memory_space=pltpu.VMEM)
    anywhere = pl.BlockSpec(memory_space=pl.ANY)
    buffers = [
        ((model_width, units), bf16), ((model_width, units), bf16), ((units, model_width), bf16),
        (output_weight.shape, bf16), ((HK, HV), bf16), ((places - 1, HK, HV), bf16),
        ((8, HK), f32), ((places - 1, 8, HK), f32), ((tokens, HV), f32),
        ((shares, tokens, cols), bf16), ((shares - 1, tokens, cols), bf16), ((tokens, cols), f32),
        ((places, shares, tokens, cols), bf16), ((8, tokens), f32), ((shares - 1, 8, tokens), f32),
        ((places, 8, tokens), f32),
        ((places, 2, tokens, cols), bf16), ((places, 2, tokens, cols), bf16),
        ((places, 2, tokens, cols), f32),
        ((places, tokens, cols), bf16), ((places, tokens, cols), bf16),
        ((places, tokens, cols), bf16), ((places, tokens, cols), bf16),
    ]
    far = places - 1
    counts = [(4,)]
    for count in (
        (far, 3), (copies - 1, far, 3), (far,), (far,), (shares - 1,), (shares - 1,), (far,), (far,),
        (places,), (places,), (places,), (places,), (places,), (places,),
    ):
        counts += [count, count]
    kernel = functools.partial(fused_kernel, places, shares, copies, units)
    return pl.pallas_call(
        kernel,
        out_shape=jax.ShapeDtypeStruct((tokens, cols), bf16),
        in_specs=[vmem] * 9 + [anywhere] * 4,
        out_specs=vmem,
        scratch_shapes=[pltpu.VMEM(shape, kind) for shape, kind in buffers]
        + [pltpu.SemaphoreType.DMA(count) for count in counts],
        compiler_params=pltpu.CompilerParams(
            collective_id=0, has_side_effects=True, vmem_limit_bytes=58 * 1024 * 1024
        ),
    )(
        stream, queries, key_matrix, value_matrix, output_gate_logits, forgetting_raw_score,
        additional_forgetting_rate, head_norm_gain.reshape(1, -1), feedforward_norm_gain.reshape(1, -1),
        output_weight, gate_weight, up_weight, down_weight,
    )


def spread_width(stream, queries, gate_weight):
    places, shares, copies = (lax.axis_size(a) for a in ("sp", "tp", "grp"))
    tokens, model_width = stream.shape
    depth, hidden_share = gate_weight.shape
    units = -(-hidden_share // (places * 128)) * 128
    fits = (
        shares == 4 and places > 1 and copies > 1 and queries.shape[1] == HK
        and tokens % 128 == 0 and model_width % (shares * 128) == 0 and depth % (copies * 128) == 0
        and hidden_share % 128 == 0 and places * units - hidden_share < units
        and 2 * tokens * places < 3 * hidden_share
    )
    return units if fits else 0


def local(
    stream,
    queries,
    key_matrix,
    value_matrix,
    output_gate_logits,
    forgetting_raw_score,
    additional_forgetting_rate,
    head_norm_gain,
    output_weight,
    feedforward_norm_gain,
    gate_weight,
    up_weight,
    down_weight,
):
    units = spread_width(stream, queries, gate_weight)
    if units:
        return fused(
            units, stream, queries, key_matrix, value_matrix, output_gate_logits,
            forgetting_raw_score, additional_forgetting_rate, head_norm_gain, output_weight,
            feedforward_norm_gain, gate_weight, up_weight, down_weight,
        )
    tokens = queries.shape[0]
    owned_heads = queries.shape[1] // HK
    blocks = tokens // BLOCK
    forgetting_exponent = (
        jax.nn.log_sigmoid(forgetting_raw_score) / sigmoid_sharpness + additional_forgetting_rate
    )
    query_part = split_heads(queries, blocks, owned_heads, HK) * HK ** (-0.5)
    key_part = split_heads(key_matrix, blocks, owned_heads, HK)
    value_part = split_heads(value_matrix, blocks, owned_heads, HV)
    decay_part = split_heads(forgetting_exponent, blocks, owned_heads, HK)
    within = jnp.cumsum(decay_part, axis=2)
    closing = within[:, :, -1, :]
    query_in = query_part * jnp.exp(within)
    key_in = key_part * jnp.exp(-within)
    key_end = key_part * jnp.exp(closing[:, :, None, :] - within)
    causal = jnp.tril(jnp.ones((BLOCK, BLOCK), jnp.bool_))
    scores = jnp.einsum("hntd,hnsd->hnts", query_in, key_in, precision=highest)
    scores = jnp.where(causal, scores, 0.0)
    inside = jnp.einsum("hnts,hnsv->hntv", scores, value_part, precision=highest)

    def advance(memory, inputs):
        query_block, key_block, value_block, decay_block = inputs
        final_answer = jnp.einsum("htd,hdv->htv", query_block, memory, precision=highest)
        memory = decay_block[:, :, None] * memory + jnp.einsum(
            "hsd,hsv->hdv", key_block, value_block, precision=highest
        )
        return (memory, final_answer)

    sequence = (
        jnp.moveaxis(query_in, 1, 0),
        jnp.moveaxis(key_end, 1, 0),
        jnp.moveaxis(value_part, 1, 0),
        jnp.moveaxis(jnp.exp(closing), 1, 0),
    )
    start_memory = jnp.zeros((owned_heads, HK, HV), jnp.float32)
    final_memory, earlier_blocks = lax.scan(advance, start_memory, sequence)
    device_decay = jnp.exp(jnp.sum(closing, axis=1))
    neutral = (jnp.ones_like(device_decay), jnp.zeros_like(final_memory))
    _, carried = carried_in((device_decay, final_memory), "sp", combine, neutral)
    before = jnp.cumsum(closing, axis=1) - closing
    query_far = query_in * jnp.exp(before[:, :, None, :])
    outside = jnp.einsum("hntd,hdv->hntv", query_far, carried, precision=highest)
    mixed_heads = inside + jnp.moveaxis(earlier_blocks, 0, 1) + outside
    mixed_heads = mixed_heads.transpose(1, 2, 0, 3).reshape(tokens, owned_heads, HV)
    mixed_heads = mixed_heads * lax.rsqrt(
        jnp.mean(mixed_heads * mixed_heads, axis=-1, keepdims=True) + epsilon
    )
    gated_rows = (
        mixed_heads.reshape(tokens, owned_heads * HV)
        * head_norm_gain
        * jax.nn.silu(output_gate_logits.astype(jnp.float32))
    ).astype(jnp.bfloat16)
    partial_out = jnp.dot(gated_rows, output_weight, preferred_element_type=jnp.float32)
    model_width = stream.shape[1]
    column_share = model_width // lax.axis_size("tp")
    column_start = lax.axis_index("tp") * column_share
    attn_cols = lax.psum_scatter(
        partial_out.astype(jnp.bfloat16), "tp", scatter_dimension=1, tiled=True
    ).astype(jnp.float32)
    resid_part = (
        lax.dynamic_slice_in_dim(stream, column_start, column_share, 1).astype(jnp.float32)
        + attn_cols
    )
    elementwise_power = lax.psum(jnp.sum(resid_part * resid_part, axis=1), "tp")
    gain_part = lax.dynamic_slice_in_dim(
        feedforward_norm_gain, column_start, column_share, 0
    ).astype(jnp.float32)
    rescaled_portion = (
        resid_part * lax.rsqrt(elementwise_power / model_width + epsilon)[:, None] * gain_part
    ).astype(jnp.bfloat16)
    normed = lax.all_gather(rescaled_portion, "tp", axis=1, tiled=True)
    gate_sum = jnp.dot(
        normed,
        lax.all_gather(gate_weight, "sp", axis=0, tiled=True),
        preferred_element_type=jnp.float32,
    )
    up_sum = jnp.dot(
        normed,
        lax.all_gather(up_weight, "sp", axis=0, tiled=True),
        preferred_element_type=jnp.float32,
    )
    hidden = (jax.nn.silu(gate_sum) * up_sum).astype(jnp.bfloat16)
    down_sum = jnp.dot(
        hidden,
        lax.all_gather(down_weight, "sp", axis=1, tiled=True),
        preferred_element_type=jnp.float32,
    )
    ffn_part = lax.psum_scatter(
        down_sum.astype(jnp.bfloat16), "tp", scatter_dimension=1, tiled=True
    ).astype(jnp.float32)
    return (resid_part + ffn_part).astype(jnp.bfloat16)


def solution(mesh):
    return jax.shard_map(
        local,
        mesh=mesh,
        in_specs=(
            P(("grp", "sp"), None),
            P(("grp", "sp"), "tp"),
            P(("grp", "sp"), "tp"),
            P(("grp", "sp"), "tp"),
            P(("grp", "sp"), "tp"),
            P(("grp", "sp"), "tp"),
            P(("grp", "sp"), "tp"),
            P("tp"),
            P("tp", None),
            P(),
            P("sp", "tp"),
            P("sp", "tp"),
            P("tp", "sp"),
        ),
        out_specs=P(("grp", "sp"), "tp"),
        check_vma=False,
    )
```

```python
import functools
import jax
import jax.numpy as jnp
from jax import lax
from jax.sharding import PartitionSpec as P
from jax.experimental import pallas as pl
from jax.experimental.pallas import tpu as pltpu

HK = 256
HV = 512
BLOCK = 64


epsilon = 1e-06
sigmoid_sharpness = 16.0
highest = lax.Precision.HIGHEST


def carried_in(value, axis, join, neutral):
    place = lax.axis_index(axis)
    gathered = jax.tree.map(
        lambda a, kind: lax.all_gather(a.astype(kind), axis), value, (jnp.bfloat16, jnp.bfloat16)
    )
    state = jax.tree.map(lambda a, e: jnp.zeros_like(a) + jnp.asarray(e, a.dtype), value, neutral)

    def one(turn, state):
        return join(
            state,
            jax.tree.map(
                lambda a, own: lax.dynamic_index_in_dim(a, turn, 0, False).astype(own.dtype),
                gathered,
                value,
            ),
        )

    return lax.fori_loop(0, place, one, state)


def split_heads(tensor, blocks, count, depth):
    return tensor.astype(jnp.float32).reshape(blocks, BLOCK, count, depth).transpose(2, 0, 1, 3)


def combine(earlier, later):
    return (earlier[0] * later[0], later[0][:, :, None] * earlier[1] + later[1])


def nt_dot(a, b):
    return lax.dot_general(a, b, (((1,), (1,)), ((), ())), preferred_element_type=jnp.float32)


def fused_kernel(
    places, shares, copies, units,
    stream, queries, keys, values, out_gate, raw_score, extra_rate, head_gain, ffn_gain,
    out_weight, gate_weight, up_weight, down_weight,
    out,
    gate_buf, up_buf, down_buf, wo_buf, state_own, state_out, state_in, hidden_all, attn,
    proj_out, proj_in, resid, y_all, square_own, square_in, total,
    pair_out, pair_in, held, cross_out, cross_in, line_out, line_in,
    local_sem, wide_send, wide_recv, pass_send, pass_recv, state_send, state_recv,
    proj_send, proj_recv, square_send, square_recv,
    total_send, total_recv, up_send, up_recv, down_send, down_recv, core_send, core_recv,
    chip_send, chip_recv, relay_send, relay_recv, pair_send, pair_recv,
    cross_send, cross_recv, sum_send, sum_recv,
):
    s = lax.axis_index("sp")
    t = lax.axis_index("tp")
    g = lax.axis_index("grp")
    f32, bf16 = jnp.float32, jnp.bfloat16
    tokens = queries.shape[0]
    cols = out.shape[1]
    model_width = stream.shape[1]
    depth = gate_weight.shape[0]
    part = depth // copies
    excess = places * units - gate_weight.shape[1]
    blocks = tokens // BLOCK

    def send(src, dst, send_sem, recv_sem, **where):
        return pltpu.make_async_remote_copy(
            src_ref=src, dst_ref=dst, send_sem=send_sem, recv_sem=recv_sem,
            device_id=where, device_id_type=pl.DeviceIdType.MESH,
        )

    def up_by(k):
        return lax.rem(s + k, places)

    def down_by(k):
        return lax.rem(s + places - k, places)

    short = units - excess

    weights = ((gate_weight, gate_buf), (up_weight, up_buf), (down_weight, down_buf))

    def region(m, source, copy, size):
        at = pl.ds(pl.multiple_of(source * depth + copy * part, 128), size)
        return weights[m][1].at[:, at] if m == 2 else weights[m][1].at[at, :]

    def taken(m, ref, size):
        return ref.at[0:size, :] if m == 2 else ref.at[:, 0:size]

    def source_of(m, target, copy, size, width):
        at = pl.ds(pl.multiple_of(copy * part, 128), size)
        back = target // (places - 1) * excess if width == units else 0
        chosen = pl.ds(pl.multiple_of(target * units - back, 128), width)
        return weights[m][0].at[chosen, at] if m == 2 else weights[m][0].at[at, chosen]

    def wide_copy(k, m, width):
        return send(
            source_of(m, up_by(k), g, part, width), taken(m, region(m, s, g, part), width),
            wide_send.at[k - 1, m], wide_recv.at[k - 1, m], sp=up_by(k),
        )

    def pass_copy(k, m, turn, width):
        here = taken(m, region(m, down_by(k), g, part), width)
        return send(
            here, here, pass_send.at[turn - 1, k - 1, m], pass_recv.at[turn - 1, k - 1, m],
            grp=lax.rem(g + turn, copies),
        )

    def own_copy(m, width):
        return pltpu.make_async_copy(
            source_of(m, s, 0, depth, width), taken(m, region(m, s, 0, depth), width), local_sem.at[m]
        )

    def by_width(place, act):
        if excess == 0:
            act(units)
            return

        @pl.when(place == places - 1)
        def _():
            act(short)

        @pl.when(place != places - 1)
        def _():
            act(units)

    def wide_start(k, m):
        by_width(up_by(k), lambda width: wide_copy(k, m, width).start())

    def wide_sent(k, m):
        by_width(up_by(k), lambda width: wide_copy(k, m, width).wait_send())

    def arrive_and_pass(k, m):
        def act(width):
            wide_copy(k, m, width).wait_recv()
            for turn in range(1, copies):
                pass_copy(k, m, turn, width).start()

        by_width(s, act)

    def pass_arrive(m):
        def act(width):
            own_copy(m, width).wait()
            for k in range(1, places):
                for turn in range(1, copies):
                    pass_copy(k, m, turn, width).wait_recv()

        by_width(s, act)

    def pass_sent(m):
        def act(width):
            for k in range(1, places):
                for turn in range(1, copies):
                    pass_copy(k, m, turn, width).wait_send()

        by_width(s, act)

    def start_upward(k, m):
        @pl.when(s + k < places)
        def _():
            wide_start(k, m)

    def start_downward(k, m):
        @pl.when(s + k >= places)
        def _():
            wide_start(k, m)

    load_out = pltpu.make_async_copy(out_weight, wo_buf, local_sem.at[3])
    load_out.start()

    def own_start(width):
        for m in range(3):
            own_copy(m, width).start()

    by_width(s, own_start)
    if excess > 0:

        @pl.when(s == places - 1)
        def _():
            gate_buf[:, short:] = jnp.zeros((model_width, excess), bf16)
            up_buf[:, short:] = jnp.zeros((model_width, excess), bf16)
            down_buf[short:, :] = jnp.zeros((excess, model_width), bf16)

    barrier = pltpu.get_barrier_semaphore()
    for k in range(1, places):
        pl.semaphore_signal(barrier, inc=1, device_id={"sp": up_by(k)}, device_id_type=pl.DeviceIdType.MESH)
    for j in range(1, shares):
        pl.semaphore_signal(
            barrier, inc=1, device_id={"tp": lax.rem(t + j, shares)}, device_id_type=pl.DeviceIdType.MESH
        )
    for j in range(1, copies):
        pl.semaphore_signal(
            barrier, inc=1, device_id={"grp": lax.rem(g + j, copies)}, device_id_type=pl.DeviceIdType.MESH
        )
    pl.semaphore_wait(barrier, places + shares + copies - 3)

    far_first = list(range(places // 2, places)) + list(range(1, places // 2))
    start_upward(far_first[0], 0)
    for m in range(2):
        for k in range(places - 1, 0, -1):
            start_downward(k, m)

    score = raw_score[...]
    decay = (
        -(jnp.maximum(-score, 0.0) + jnp.log1p(jnp.exp(-jnp.abs(score)))) / sigmoid_sharpness
        + extra_rate[...]
    )
    row = lax.broadcasted_iota(jnp.int32, (tokens, tokens), 0)
    col = lax.broadcasted_iota(jnp.int32, (tokens, tokens), 1)
    causal = row >= col
    running = jnp.dot(
        jnp.where(causal, 1.0, 0.0), decay, precision=highest, preferred_element_type=f32
    )
    last = running[tokens - 1 : tokens, :]
    key = keys[...].astype(f32)
    value = values[...]
    key_end = (key * jnp.exp(last - running)).astype(bf16)
    state_own[...] = lax.dot_general(
        key_end, value, (((0,), (0,)), ((), ())), preferred_element_type=f32
    )
    kept = jnp.exp(
        lax.dot_general(
            decay, jnp.ones((tokens, 128), f32), (((0,), (0,)), ((), ())),
            precision=highest, preferred_element_type=f32,
        )
    )
    chunks = state_out.shape[0]

    def state_copy(c):
        return send(
            state_out.at[c], state_in.at[c], state_send.at[c], state_recv.at[c],
            sp=lax.rem(s + 1, places),
        )

    @pl.when(s == 0)
    def _():
        for c in range(chunks):
            state_out[c] = state_own[:, c * 128 : (c + 1) * 128].astype(bf16)
            state_copy(c).start()

    query = queries[...].astype(f32) * HK ** (-0.5)
    pieces = []
    for b in range(blocks):
        rows = slice(b * BLOCK, (b + 1) * BLOCK)
        begin = jnp.zeros_like(last) if b == 0 else running[b * BLOCK - 1 : b * BLOCK, :]
        inner = running[rows] - begin
        scores = nt_dot(
            (query[rows] * jnp.exp(inner)).astype(bf16), (key[rows] * jnp.exp(-inner)).astype(bf16)
        )
        scores = jnp.where(causal[:BLOCK, :BLOCK], scores, 0.0).astype(bf16)
        piece = jnp.dot(scores, value[rows], preferred_element_type=f32)
        for c in range(b):
            old = slice(c * BLOCK, (c + 1) * BLOCK)
            close = running[(c + 1) * BLOCK - 1 : (c + 1) * BLOCK, :]
            far = nt_dot(
                (query[rows] * jnp.exp(running[rows] - close)).astype(bf16),
                (key[old] * jnp.exp(close - running[old])).astype(bf16),
            )
            piece = piece + jnp.dot(far.astype(bf16), value[old], preferred_element_type=f32)
        attn[rows, :] = piece

    logits = out_gate[...].astype(f32)
    gate_factor = head_gain[...] * (logits / (1.0 + jnp.exp(-logits)))
    query_far = query * jnp.exp(running)
    far_query = query_far.astype(bf16)

    @pl.when(s > 0)
    def _():
        for c in range(chunks):
            here = slice(c * 128, (c + 1) * 128)
            state_copy(c).wait_recv()

            @pl.when(s < places - 1)
            def _():
                state_out[c] = (kept * state_in[c].astype(f32) + state_own[:, here]).astype(bf16)
                state_copy(c).start()

        for c in range(chunks):
            here = slice(c * 128, (c + 1) * 128)
            attn[:, here] += jnp.dot(far_query, state_in[c], preferred_element_type=f32)

    for k in far_first[1:]:
        start_upward(k, 0)
    for k in far_first:
        start_upward(k, 1)

    heads = attn[...]
    heads = heads * lax.rsqrt(jnp.mean(heads * heads, axis=-1, keepdims=True) + epsilon)
    gated = (heads * gate_factor).astype(bf16)
    load_out.wait()

    def columns(i):
        return pl.ds(pl.multiple_of(i * cols, 128), cols)

    def proj_copy(j):
        target = lax.rem(t + j, shares)
        return send(
            proj_out.at[j], proj_in.at[j - 1], proj_send.at[j - 1], proj_recv.at[j - 1], tp=target
        )

    for j in (2, 3, 1, 0) if shares == 4 else range(shares - 1, -1, -1):
        target = lax.rem(t + j, shares)
        proj_out[j] = jnp.dot(gated, wo_buf[:, columns(target)], preferred_element_type=f32).astype(bf16)
        if j > 0:
            proj_copy(j).start()

    joined = proj_out[0].astype(f32)
    for j in range(1, shares):
        proj_copy(j).wait_recv()
        joined = joined + proj_in[j - 1].astype(f32)
    joined = stream[:, columns(t)].astype(f32) + joined
    resid[...] = joined
    square_own[...] = lax.dot_general(
        jnp.ones((8, cols), f32), joined * joined, (((1,), (1,)), ((), ())),
        precision=highest, preferred_element_type=f32,
    )
    y_all[s, t] = (joined * ffn_gain[:, columns(t)].astype(f32)).astype(bf16)

    def square_copy(j):
        return send(
            square_own, square_in.at[j - 1], square_send.at[j - 1], square_recv.at[j - 1],
            tp=lax.rem(t + j, shares),
        )

    def total_copy(k):
        return send(total.at[0], total.at[k], total_send.at[k - 1], total_recv.at[k - 1], sp=up_by(k))

    def up_y(k):
        held_y = y_all.at[down_by(k - 1), t]
        return send(held_y, held_y, up_send.at[k - 1], up_recv.at[k - 1], sp=lax.rem(s + 1, places))

    def down_y(k):
        held_y = y_all.at[up_by(k - 1), t]
        return send(
            held_y, held_y, down_send.at[k - 1], down_recv.at[k - 1], sp=lax.rem(s + places - 1, places)
        )

    def pass_up(k, finish=False):
        @pl.when(jnp.logical_and(s + 1 < places, s >= k - 1))
        def _():
            if finish:
                up_y(k).wait_send()
            else:
                up_y(k).start()

    def pass_down(k, finish=False):
        @pl.when(jnp.logical_and(s >= 1, s + k - 1 < places))
        def _():
            if finish:
                down_y(k).wait_send()
            else:
                down_y(k).start()

    half = shares // 2
    near = t + 1 - 2 * lax.rem(t, 2)
    across = lax.rem(t + half, shares)
    diagonal = lax.rem(near + half, shares)

    def core_y(k):
        held_y = y_all.at[down_by(k), t]
        return send(held_y, held_y, core_send.at[k], core_recv.at[k], tp=near)

    def chip_y(k):
        held_y = y_all.at[down_by(k), t]
        return send(held_y, held_y, chip_send.at[k], chip_recv.at[k], tp=across)

    def relay_y(k):
        held_y = y_all.at[down_by(k), across]
        return send(held_y, held_y, relay_send.at[k], relay_recv.at[k], tp=near)

    for j in range(1, shares):
        square_copy(j).start()
    pass_up(1)
    pass_down(1)
    chip_y(0).start()
    core_y(0).start()
    for k in range(1, places):
        wide_start(far_first[k - 1], 2)
    for k in range(1, places):
        arrive_and_pass(k, 0)
    squares = square_own[...]
    for j in range(1, shares):
        square_copy(j).wait_recv()
        squares = squares + square_in[j - 1]
    total[0] = squares
    for k in range(1, places):
        total_copy(k).start()
    for k in range(1, places):
        arrive_and_pass(k, 1)
    chip_y(0).wait_recv()
    relay_y(0).start()
    for k in range(1, places):

        @pl.when(s >= k)
        def _():
            up_y(k).wait_recv()
            if k + 1 < places:
                pass_up(k + 1)
            chip_y(k).start()
            core_y(k).start()

        @pl.when(s + k < places)
        def _():
            down_y(k).wait_recv()
            if k + 1 < places:
                pass_down(k + 1)
            chip_y(places - k).start()
            core_y(places - k).start()

    for k in range(1, places):
        chip_y(k).wait_recv()
        relay_y(k).start()
    for m in range(2):
        pass_arrive(m)
    unit_at = lax.broadcasted_iota(jnp.int32, (tokens, units), 1)
    keep = unit_at < units - (s // (places - 1)) * excess
    identity = jnp.where(row == col, 1.0, 0.0)

    def pair_copy(k):
        return send(pair_out.at[k], pair_in.at[k], pair_send.at[k], pair_recv.at[k], tp=near)

    def cross_copy(k):
        return send(cross_out.at[k], cross_in.at[k], cross_send.at[k], cross_recv.at[k], tp=across)

    def sum_copy(k):
        return send(line_out.at[k], line_in.at[k], sum_send.at[k], sum_recv.at[k], sp=down_by(k))

    def pair_step(k):
        pair_copy(k).wait_recv()
        cross_out[k] = (held[k, 1] + pair_in[k, 1].astype(f32)).astype(bf16)
        cross_copy(k).start()
        held[k, 0] = held[k, 0] + pair_in[k, 0].astype(f32)

    def cross_step(k):
        cross_copy(k).wait_recv()
        if k == 0:
            held[k, 0] = held[k, 0] + cross_in[k].astype(f32)
        else:
            line_out[k] = (held[k, 0] + cross_in[k].astype(f32)).astype(bf16)
            sum_copy(k).start()

    order = list(range(1, places)) + [0]
    for turn_at, k in enumerate([0] + list(range(1, places))):
        block = down_by(k)
        core_y(k).wait_recv()
        relay_y(k).wait_recv()
        if k > 0:
            total_copy(k).wait_recv()
        scale = lax.dot_general(
            identity, total[k], (((1,), (1,)), ((), ())), precision=highest, preferred_element_type=f32
        )[:, 0:1]
        scale = lax.rsqrt(scale / model_width + epsilon)
        gate_sum = jnp.zeros((tokens, units), f32)
        up_sum = jnp.zeros((tokens, units), f32)
        for i in range(shares):
            y = y_all[block, i]
            here = slice(i * cols, (i + 1) * cols)
            gate_sum = gate_sum + jnp.dot(y, gate_buf[here, :], preferred_element_type=f32)
            up_sum = up_sum + jnp.dot(y, up_buf[here, :], preferred_element_type=f32)
        gate_sum = gate_sum * scale
        up_sum = up_sum * scale
        hidden = gate_sum / (1.0 + jnp.exp(-gate_sum)) * up_sum
        hidden_all[k] = jnp.where(keep, hidden, 0.0).astype(bf16)
        if k > 0:
            arrive_and_pass(k, 2)
    pass_arrive(2)
    for turn_at, k in enumerate(order):
        hidden = hidden_all[k]
        for i, target in enumerate((near, diagonal)):
            pair_out[k, i] = jnp.dot(
                hidden, down_buf[:, columns(target)], preferred_element_type=f32
            ).astype(bf16)
        pair_copy(k).start()
        for i, target in enumerate((t, across)):
            held[k, i] = jnp.dot(hidden, down_buf[:, columns(target)], preferred_element_type=f32)
        if turn_at > 0:
            pair_step(order[turn_at - 1])
        if turn_at > 1:
            cross_step(order[turn_at - 2])
    pair_step(order[-1])
    for k in order[-2:]:
        cross_step(k)
    result = resid[...] + held[0, 0]
    for k in range(1, places):
        sum_copy(k).wait_recv()
        result = result + line_in[k].astype(f32)
    out[...] = result.astype(bf16)

    @pl.when(s < places - 1)
    def _():
        for c in range(chunks):
            state_copy(c).wait_send()

    for k in range(1, places):
        for m in range(3):
            wide_sent(k, m)
        pass_up(k, True)
        pass_down(k, True)
        total_copy(k).wait_send()
        sum_copy(k).wait_send()
    for m in range(3):
        pass_sent(m)
    for j in range(1, shares):
        proj_copy(j).wait_send()
        square_copy(j).wait_send()
    for k in range(places):
        for copy in (core_y, chip_y, relay_y, pair_copy, cross_copy):
            copy(k).wait_send()


def fused(units, *arrays):
    (
        stream, queries, key_matrix, value_matrix, output_gate_logits, forgetting_raw_score,
        additional_forgetting_rate, head_norm_gain, output_weight, feedforward_norm_gain,
        gate_weight, up_weight, down_weight,
    ) = arrays
    places, shares, copies = (lax.axis_size(a) for a in ("sp", "tp", "grp"))
    tokens, model_width = stream.shape
    cols = model_width // shares
    f32, bf16 = jnp.float32, jnp.bfloat16
    vmem = pl.BlockSpec(memory_space=pltpu.VMEM)
    anywhere = pl.BlockSpec(memory_space=pl.ANY)
    buffers = [
        ((model_width, units), bf16), ((model_width, units), bf16), ((units, model_width), bf16),
        (output_weight.shape, bf16), ((HK, HV), f32), ((HV // 128, HK, 128), bf16),
        ((HV // 128, HK, 128), bf16), ((places, tokens, units), bf16), ((tokens, HV), f32),
        ((shares, tokens, cols), bf16), ((shares - 1, tokens, cols), bf16), ((tokens, cols), f32),
        ((places, shares, tokens, cols), bf16), ((8, tokens), f32), ((shares - 1, 8, tokens), f32),
        ((places, 8, tokens), f32),
        ((places, 2, tokens, cols), bf16), ((places, 2, tokens, cols), bf16),
        ((places, 2, tokens, cols), f32),
        ((places, tokens, cols), bf16), ((places, tokens, cols), bf16),
        ((places, tokens, cols), bf16), ((places, tokens, cols), bf16),
    ]
    far = places - 1
    counts = [(4,)]
    for count in (
        (far, 3), (copies - 1, far, 3), (HV // 128,), (shares - 1,), (shares - 1,), (far,), (far,), (far,),
        (places,), (places,), (places,), (places,), (places,), (places,),
    ):
        counts += [count, count]
    kernel = functools.partial(fused_kernel, places, shares, copies, units)
    return pl.pallas_call(
        kernel,
        out_shape=jax.ShapeDtypeStruct((tokens, cols), bf16),
        in_specs=[vmem] * 9 + [anywhere] * 4,
        out_specs=vmem,
        scratch_shapes=[pltpu.VMEM(shape, kind) for shape, kind in buffers]
        + [pltpu.SemaphoreType.DMA(count) for count in counts],
        compiler_params=pltpu.CompilerParams(
            collective_id=0, has_side_effects=True, vmem_limit_bytes=58 * 1024 * 1024
        ),
    )(
        stream, queries, key_matrix, value_matrix, output_gate_logits, forgetting_raw_score,
        additional_forgetting_rate, head_norm_gain.reshape(1, -1), feedforward_norm_gain.reshape(1, -1),
        output_weight, gate_weight, up_weight, down_weight,
    )


def spread_width(stream, queries, gate_weight):
    places, shares, copies = (lax.axis_size(a) for a in ("sp", "tp", "grp"))
    tokens, model_width = stream.shape
    depth, hidden_share = gate_weight.shape
    units = -(-hidden_share // (places * 128)) * 128
    fits = (
        shares == 4 and places > 1 and copies > 1 and queries.shape[1] == HK
        and tokens % 128 == 0 and model_width % (shares * 128) == 0 and depth % (copies * 128) == 0
        and hidden_share % 128 == 0 and places * units - hidden_share < units
        and 2 * tokens * places < 3 * hidden_share
    )
    return units if fits else 0


def local(
    stream,
    queries,
    key_matrix,
    value_matrix,
    output_gate_logits,
    forgetting_raw_score,
    additional_forgetting_rate,
    head_norm_gain,
    output_weight,
    feedforward_norm_gain,
    gate_weight,
    up_weight,
    down_weight,
):
    units = spread_width(stream, queries, gate_weight)
    if units:
        return fused(
            units, stream, queries, key_matrix, value_matrix, output_gate_logits,
            forgetting_raw_score, additional_forgetting_rate, head_norm_gain, output_weight,
            feedforward_norm_gain, gate_weight, up_weight, down_weight,
        )
    tokens = queries.shape[0]
    owned_heads = queries.shape[1] // HK
    blocks = tokens // BLOCK
    forgetting_exponent = (
        jax.nn.log_sigmoid(forgetting_raw_score) / sigmoid_sharpness + additional_forgetting_rate
    )
    query_part = split_heads(queries, blocks, owned_heads, HK) * HK ** (-0.5)
    key_part = split_heads(key_matrix, blocks, owned_heads, HK)
    value_part = split_heads(value_matrix, blocks, owned_heads, HV)
    decay_part = split_heads(forgetting_exponent, blocks, owned_heads, HK)
    within = jnp.cumsum(decay_part, axis=2)
    closing = within[:, :, -1, :]
    query_in = query_part * jnp.exp(within)
    key_in = key_part * jnp.exp(-within)
    key_end = key_part * jnp.exp(closing[:, :, None, :] - within)
    causal = jnp.tril(jnp.ones((BLOCK, BLOCK), jnp.bool_))
    scores = jnp.einsum("hntd,hnsd->hnts", query_in, key_in, precision=highest)
    scores = jnp.where(causal, scores, 0.0)
    inside = jnp.einsum("hnts,hnsv->hntv", scores, value_part, precision=highest)

    def advance(memory, inputs):
        query_block, key_block, value_block, decay_block = inputs
        final_answer = jnp.einsum("htd,hdv->htv", query_block, memory, precision=highest)
        memory = decay_block[:, :, None] * memory + jnp.einsum(
            "hsd,hsv->hdv", key_block, value_block, precision=highest
        )
        return (memory, final_answer)

    sequence = (
        jnp.moveaxis(query_in, 1, 0),
        jnp.moveaxis(key_end, 1, 0),
        jnp.moveaxis(value_part, 1, 0),
        jnp.moveaxis(jnp.exp(closing), 1, 0),
    )
    start_memory = jnp.zeros((owned_heads, HK, HV), jnp.float32)
    final_memory, earlier_blocks = lax.scan(advance, start_memory, sequence)
    device_decay = jnp.exp(jnp.sum(closing, axis=1))
    neutral = (jnp.ones_like(device_decay), jnp.zeros_like(final_memory))
    _, carried = carried_in((device_decay, final_memory), "sp", combine, neutral)
    before = jnp.cumsum(closing, axis=1) - closing
    query_far = query_in * jnp.exp(before[:, :, None, :])
    outside = jnp.einsum("hntd,hdv->hntv", query_far, carried, precision=highest)
    mixed_heads = inside + jnp.moveaxis(earlier_blocks, 0, 1) + outside
    mixed_heads = mixed_heads.transpose(1, 2, 0, 3).reshape(tokens, owned_heads, HV)
    mixed_heads = mixed_heads * lax.rsqrt(
        jnp.mean(mixed_heads * mixed_heads, axis=-1, keepdims=True) + epsilon
    )
    gated_rows = (
        mixed_heads.reshape(tokens, owned_heads * HV)
        * head_norm_gain
        * jax.nn.silu(output_gate_logits.astype(jnp.float32))
    ).astype(jnp.bfloat16)
    partial_out = jnp.dot(gated_rows, output_weight, preferred_element_type=jnp.float32)
    model_width = stream.shape[1]
    column_share = model_width // lax.axis_size("tp")
    column_start = lax.axis_index("tp") * column_share
    attn_cols = lax.psum_scatter(
        partial_out.astype(jnp.bfloat16), "tp", scatter_dimension=1, tiled=True
    ).astype(jnp.float32)
    resid_part = (
        lax.dynamic_slice_in_dim(stream, column_start, column_share, 1).astype(jnp.float32)
        + attn_cols
    )
    elementwise_power = lax.psum(jnp.sum(resid_part * resid_part, axis=1), "tp")
    gain_part = lax.dynamic_slice_in_dim(
        feedforward_norm_gain, column_start, column_share, 0
    ).astype(jnp.float32)
    rescaled_portion = (
        resid_part * lax.rsqrt(elementwise_power / model_width + epsilon)[:, None] * gain_part
    ).astype(jnp.bfloat16)
    normed = lax.all_gather(rescaled_portion, "tp", axis=1, tiled=True)
    gate_sum = jnp.dot(
        normed,
        lax.all_gather(gate_weight, "sp", axis=0, tiled=True),
        preferred_element_type=jnp.float32,
    )
    up_sum = jnp.dot(
        normed,
        lax.all_gather(up_weight, "sp", axis=0, tiled=True),
        preferred_element_type=jnp.float32,
    )
    hidden = (jax.nn.silu(gate_sum) * up_sum).astype(jnp.bfloat16)
    down_sum = jnp.dot(
        hidden,
        lax.all_gather(down_weight, "sp", axis=1, tiled=True),
        preferred_element_type=jnp.float32,
    )
    ffn_part = lax.psum_scatter(
        down_sum.astype(jnp.bfloat16), "tp", scatter_dimension=1, tiled=True
    ).astype(jnp.float32)
    return (resid_part + ffn_part).astype(jnp.bfloat16)


def solution(mesh):
    return jax.shard_map(
        local,
        mesh=mesh,
        in_specs=(
            P(("grp", "sp"), None),
            P(("grp", "sp"), "tp"),
            P(("grp", "sp"), "tp"),
            P(("grp", "sp"), "tp"),
            P(("grp", "sp"), "tp"),
            P(("grp", "sp"), "tp"),
            P(("grp", "sp"), "tp"),
            P("tp"),
            P("tp", None),
            P(),
            P("sp", "tp"),
            P("sp", "tp"),
            P("tp", "sp"),
        ),
        out_specs=P(("grp", "sp"), "tp"),
        check_vma=False,
    )
```

```python
import functools
import jax
import jax.numpy as jnp
from jax import lax
from jax.sharding import PartitionSpec as P
from jax.experimental import pallas as pl
from jax.experimental.pallas import tpu as pltpu

HK = 256
HV = 512
BLOCK = 64


epsilon = 1e-06
sigmoid_sharpness = 16.0
highest = lax.Precision.HIGHEST


def carried_in(value, axis, join, neutral):
    place = lax.axis_index(axis)
    gathered = jax.tree.map(
        lambda a, kind: lax.all_gather(a.astype(kind), axis), value, (jnp.bfloat16, jnp.bfloat16)
    )
    state = jax.tree.map(lambda a, e: jnp.zeros_like(a) + jnp.asarray(e, a.dtype), value, neutral)

    def one(turn, state):
        return join(
            state,
            jax.tree.map(
                lambda a, own: lax.dynamic_index_in_dim(a, turn, 0, False).astype(own.dtype),
                gathered,
                value,
            ),
        )

    return lax.fori_loop(0, place, one, state)


def split_heads(tensor, blocks, count, depth):
    return tensor.astype(jnp.float32).reshape(blocks, BLOCK, count, depth).transpose(2, 0, 1, 3)


def combine(earlier, later):
    return (earlier[0] * later[0], later[0][:, :, None] * earlier[1] + later[1])


def nt_dot(a, b):
    return lax.dot_general(a, b, (((1,), (1,)), ((), ())), preferred_element_type=jnp.float32)


def fused_kernel(
    places, shares, copies, units,
    stream, queries, keys, values, out_gate, raw_score, extra_rate, head_gain, ffn_gain,
    out_weight, gate_weight, up_weight, down_weight,
    out,
    gate_buf, up_buf, down_buf, wo_buf, state_own, state_out, state_in, hidden_all, attn,
    proj_out, proj_in, resid, y_all, square_own, square_in, total,
    pair_out, pair_in, held, cross_out, cross_in, line_out, line_in,
    local_sem, wide_send, wide_recv, pass_send, pass_recv, state_send, state_recv,
    proj_send, proj_recv, square_send, square_recv,
    total_send, total_recv, line_y_send, line_y_recv, core_send, core_recv,
    chip_send, chip_recv, relay_send, relay_recv, pair_send, pair_recv,
    cross_send, cross_recv, sum_send, sum_recv,
):
    s = lax.axis_index("sp")
    t = lax.axis_index("tp")
    g = lax.axis_index("grp")
    f32, bf16 = jnp.float32, jnp.bfloat16
    tokens = queries.shape[0]
    cols = out.shape[1]
    model_width = stream.shape[1]
    depth = gate_weight.shape[0]
    part = depth // copies
    excess = places * units - gate_weight.shape[1]
    blocks = tokens // BLOCK

    def send(src, dst, send_sem, recv_sem, **where):
        return pltpu.make_async_remote_copy(
            src_ref=src, dst_ref=dst, send_sem=send_sem, recv_sem=recv_sem,
            device_id=where, device_id_type=pl.DeviceIdType.MESH,
        )

    def up_by(k):
        return lax.rem(s + k, places)

    def down_by(k):
        return lax.rem(s + places - k, places)

    short = units - excess

    weights = ((gate_weight, gate_buf), (up_weight, up_buf), (down_weight, down_buf))

    def region(m, source, copy, size):
        at = pl.ds(pl.multiple_of(source * depth + copy * part, 128), size)
        return weights[m][1].at[:, at] if m == 2 else weights[m][1].at[at, :]

    def taken(m, ref, size):
        return ref.at[0:size, :] if m == 2 else ref.at[:, 0:size]

    def source_of(m, target, copy, size, width):
        at = pl.ds(pl.multiple_of(copy * part, 128), size)
        back = target // (places - 1) * excess if width == units else 0
        chosen = pl.ds(pl.multiple_of(target * units - back, 128), width)
        return weights[m][0].at[chosen, at] if m == 2 else weights[m][0].at[at, chosen]

    def wide_copy(k, m, width):
        return send(
            source_of(m, up_by(k), g, part, width), taken(m, region(m, s, g, part), width),
            wide_send.at[k - 1, m], wide_recv.at[k - 1, m], sp=up_by(k),
        )

    def pass_copy(k, m, turn, width):
        here = taken(m, region(m, down_by(k), g, part), width)
        return send(
            here, here, pass_send.at[turn - 1, k - 1, m], pass_recv.at[turn - 1, k - 1, m],
            grp=lax.rem(g + turn, copies),
        )

    def own_copy(m, width):
        return pltpu.make_async_copy(
            source_of(m, s, 0, depth, width), taken(m, region(m, s, 0, depth), width), local_sem.at[m]
        )

    def by_width(place, act):
        if excess == 0:
            act(units)
            return

        @pl.when(place == places - 1)
        def _():
            act(short)

        @pl.when(place != places - 1)
        def _():
            act(units)

    def wide_start(k, m):
        by_width(up_by(k), lambda width: wide_copy(k, m, width).start())

    def wide_sent(k, m):
        by_width(up_by(k), lambda width: wide_copy(k, m, width).wait_send())

    def arrive_and_pass(k, m):
        def act(width):
            wide_copy(k, m, width).wait_recv()
            for turn in range(1, copies):
                pass_copy(k, m, turn, width).start()

        by_width(s, act)

    def pass_arrive(m):
        def act(width):
            own_copy(m, width).wait()
            for k in range(1, places):
                for turn in range(1, copies):
                    pass_copy(k, m, turn, width).wait_recv()

        by_width(s, act)

    def pass_sent(m):
        def act(width):
            for k in range(1, places):
                for turn in range(1, copies):
                    pass_copy(k, m, turn, width).wait_send()

        by_width(s, act)

    def start_upward(k, m):
        @pl.when(s + k < places)
        def _():
            wide_start(k, m)

    def start_downward(k, m):
        @pl.when(s + k >= places)
        def _():
            wide_start(k, m)

    load_out = pltpu.make_async_copy(out_weight, wo_buf, local_sem.at[3])
    load_out.start()

    def own_start(width):
        for m in range(3):
            own_copy(m, width).start()

    by_width(s, own_start)
    if excess > 0:

        @pl.when(s == places - 1)
        def _():
            gate_buf[:, short:] = jnp.zeros((model_width, excess), bf16)
            up_buf[:, short:] = jnp.zeros((model_width, excess), bf16)
            down_buf[short:, :] = jnp.zeros((excess, model_width), bf16)

    barrier = pltpu.get_barrier_semaphore()
    for k in range(1, places):
        pl.semaphore_signal(barrier, inc=1, device_id={"sp": up_by(k)}, device_id_type=pl.DeviceIdType.MESH)
    for j in range(1, shares):
        pl.semaphore_signal(
            barrier, inc=1, device_id={"tp": lax.rem(t + j, shares)}, device_id_type=pl.DeviceIdType.MESH
        )
    for j in range(1, copies):
        pl.semaphore_signal(
            barrier, inc=1, device_id={"grp": lax.rem(g + j, copies)}, device_id_type=pl.DeviceIdType.MESH
        )
    pl.semaphore_wait(barrier, places + shares + copies - 3)

    far_first = list(range(places // 2, places)) + list(range(1, places // 2))
    start_upward(far_first[0], 0)
    for m in range(2):
        for k in range(places - 1, 0, -1):
            start_downward(k, m)

    score = raw_score[...]
    decay = (
        -(jnp.maximum(-score, 0.0) + jnp.log1p(jnp.exp(-jnp.abs(score)))) / sigmoid_sharpness
        + extra_rate[...]
    )
    row = lax.broadcasted_iota(jnp.int32, (tokens, tokens), 0)
    col = lax.broadcasted_iota(jnp.int32, (tokens, tokens), 1)
    causal = row >= col
    running = jnp.dot(
        jnp.where(causal, 1.0, 0.0), decay, precision=highest, preferred_element_type=f32
    )
    last = running[tokens - 1 : tokens, :]
    key = keys[...].astype(f32)
    value = values[...]
    key_end = (key * jnp.exp(last - running)).astype(bf16)
    state_own[...] = lax.dot_general(
        key_end, value, (((0,), (0,)), ((), ())), preferred_element_type=f32
    )
    kept = jnp.exp(
        lax.dot_general(
            decay, jnp.ones((tokens, 128), f32), (((0,), (0,)), ((), ())),
            precision=highest, preferred_element_type=f32,
        )
    )
    chunks = state_out.shape[0]

    def state_copy(c):
        return send(
            state_out.at[c], state_in.at[c], state_send.at[c], state_recv.at[c],
            sp=lax.rem(s + 1, places),
        )

    @pl.when(s == 0)
    def _():
        for c in range(chunks):
            state_out[c] = state_own[:, c * 128 : (c + 1) * 128].astype(bf16)
            state_copy(c).start()

    @pl.when(s > 0)
    def _():
        for c in range(chunks):
            here = slice(c * 128, (c + 1) * 128)
            state_copy(c).wait_recv()

            @pl.when(s < places - 1)
            def _():
                state_out[c] = (kept * state_in[c].astype(f32) + state_own[:, here]).astype(bf16)
                state_copy(c).start()

    for k in far_first[1:]:
        start_upward(k, 0)
    for k in far_first:
        start_upward(k, 1)
    query = queries[...].astype(f32) * HK ** (-0.5)
    pieces = []
    for b in range(blocks):
        rows = slice(b * BLOCK, (b + 1) * BLOCK)
        begin = jnp.zeros_like(last) if b == 0 else running[b * BLOCK - 1 : b * BLOCK, :]
        inner = running[rows] - begin
        scores = nt_dot(
            (query[rows] * jnp.exp(inner)).astype(bf16), (key[rows] * jnp.exp(-inner)).astype(bf16)
        )
        scores = jnp.where(causal[:BLOCK, :BLOCK], scores, 0.0).astype(bf16)
        piece = jnp.dot(scores, value[rows], preferred_element_type=f32)
        for c in range(b):
            old = slice(c * BLOCK, (c + 1) * BLOCK)
            close = running[(c + 1) * BLOCK - 1 : (c + 1) * BLOCK, :]
            far = nt_dot(
                (query[rows] * jnp.exp(running[rows] - close)).astype(bf16),
                (key[old] * jnp.exp(close - running[old])).astype(bf16),
            )
            piece = piece + jnp.dot(far.astype(bf16), value[old], preferred_element_type=f32)
        attn[rows, :] = piece

    logits = out_gate[...].astype(f32)
    gate_factor = head_gain[...] * (logits / (1.0 + jnp.exp(-logits)))
    query_far = query * jnp.exp(running)
    far_query = query_far.astype(bf16)

    @pl.when(s > 0)
    def _():
        for c in range(chunks):
            here = slice(c * 128, (c + 1) * 128)
            attn[:, here] += jnp.dot(far_query, state_in[c], preferred_element_type=f32)

    for k in range(places - 1, 0, -1):

        @pl.when(s < k)
        def _():
            arrive_and_pass(k, 0)

    heads = attn[...]
    heads = heads * lax.rsqrt(jnp.mean(heads * heads, axis=-1, keepdims=True) + epsilon)
    gated = (heads * gate_factor).astype(bf16)
    load_out.wait()

    def columns(i):
        return pl.ds(pl.multiple_of(i * cols, 128), cols)

    def proj_copy(j):
        target = lax.rem(t + j, shares)
        return send(
            proj_out.at[j], proj_in.at[j - 1], proj_send.at[j - 1], proj_recv.at[j - 1], tp=target
        )

    for j in (2, 3, 1, 0) if shares == 4 else range(shares - 1, -1, -1):
        target = lax.rem(t + j, shares)
        proj_out[j] = jnp.dot(gated, wo_buf[:, columns(target)], preferred_element_type=f32).astype(bf16)
        if j > 0:
            proj_copy(j).start()

    joined = proj_out[0].astype(f32)
    for j in range(1, shares):
        proj_copy(j).wait_recv()
        joined = joined + proj_in[j - 1].astype(f32)
    joined = stream[:, columns(t)].astype(f32) + joined
    resid[...] = joined
    square_own[...] = lax.dot_general(
        jnp.ones((8, cols), f32), joined * joined, (((1,), (1,)), ((), ())),
        precision=highest, preferred_element_type=f32,
    )
    y_all[s, t] = (joined * ffn_gain[columns(t)].astype(f32).reshape(1, cols)).astype(bf16)

    def square_copy(j):
        return send(
            square_own, square_in.at[j - 1], square_send.at[j - 1], square_recv.at[j - 1],
            tp=lax.rem(t + j, shares),
        )

    def total_copy(k):
        return send(total.at[0], total.at[k], total_send.at[k - 1], total_recv.at[k - 1], sp=up_by(k))

    def line_y(k):
        mine = y_all.at[s, t]
        return send(mine, mine, line_y_send.at[k - 1], line_y_recv.at[k - 1], sp=up_by(k))

    half = shares // 2
    near = t + 1 - 2 * lax.rem(t, 2)
    across = lax.rem(t + half, shares)
    diagonal = lax.rem(near + half, shares)

    def core_y(k):
        held_y = y_all.at[down_by(k), t]
        return send(held_y, held_y, core_send.at[k], core_recv.at[k], tp=near)

    def chip_y(k):
        held_y = y_all.at[down_by(k), t]
        return send(held_y, held_y, chip_send.at[k], chip_recv.at[k], tp=across)

    def relay_y(k):
        held_y = y_all.at[down_by(k), across]
        return send(held_y, held_y, relay_send.at[k], relay_recv.at[k], tp=near)

    for j in range(1, shares):
        square_copy(j).start()
    for k in far_first:
        line_y(k).start()
    chip_y(0).start()
    core_y(0).start()
    for k in far_first:
        wide_start(k, 2)
    for k in range(1, places):

        @pl.when(s >= k)
        def _():
            arrive_and_pass(k, 0)

    squares = square_own[...]
    for j in range(1, shares):
        square_copy(j).wait_recv()
        squares = squares + square_in[j - 1]
    total[0] = squares
    for k in range(1, places):
        total_copy(k).start()
    for k in range(1, places):
        arrive_and_pass(k, 1)
    chip_y(0).wait_recv()
    relay_y(0).start()
    for k in range(1, places):

        @pl.when(s >= k)
        def _():
            line_y(k).wait_recv()
            chip_y(k).start()
            core_y(k).start()

        @pl.when(s + k < places)
        def _():
            line_y(places - k).wait_recv()
            chip_y(places - k).start()
            core_y(places - k).start()

    for k in range(1, places):
        chip_y(k).wait_recv()
        relay_y(k).start()
    for m in range(2):
        pass_arrive(m)
    unit_at = lax.broadcasted_iota(jnp.int32, (tokens, units), 1)
    keep = unit_at < units - (s // (places - 1)) * excess
    identity = jnp.where(row == col, 1.0, 0.0)

    def pair_copy(k):
        return send(pair_out.at[k], pair_in.at[k], pair_send.at[k], pair_recv.at[k], tp=near)

    def cross_copy(k):
        return send(cross_out.at[k], cross_in.at[k], cross_send.at[k], cross_recv.at[k], tp=across)

    def sum_copy(k):
        return send(line_out.at[k], line_in.at[k], sum_send.at[k], sum_recv.at[k], sp=down_by(k))

    def pair_step(k):
        pair_copy(k).wait_recv()
        cross_out[k] = (held[k, 1] + pair_in[k, 1].astype(f32)).astype(bf16)
        cross_copy(k).start()
        held[k, 0] = held[k, 0] + pair_in[k, 0].astype(f32)

    def cross_step(k):
        cross_copy(k).wait_recv()
        if k == 0:
            held[k, 0] = held[k, 0] + cross_in[k].astype(f32)
        else:
            line_out[k] = (held[k, 0] + cross_in[k].astype(f32)).astype(bf16)
            sum_copy(k).start()

    order = list(range(1, places)) + [0]
    for turn_at, k in enumerate([0] + list(range(1, places))):
        block = down_by(k)
        core_y(k).wait_recv()
        relay_y(k).wait_recv()
        if k > 0:
            total_copy(k).wait_recv()
        scale = lax.dot_general(
            identity, total[k], (((1,), (1,)), ((), ())), precision=highest, preferred_element_type=f32
        )[:, 0:1]
        scale = lax.rsqrt(scale / model_width + epsilon)
        gate_sum = jnp.zeros((tokens, units), f32)
        up_sum = jnp.zeros((tokens, units), f32)
        for i in range(shares):
            y = y_all[block, i]
            here = slice(i * cols, (i + 1) * cols)
            gate_sum = gate_sum + jnp.dot(y, gate_buf[here, :], preferred_element_type=f32)
            up_sum = up_sum + jnp.dot(y, up_buf[here, :], preferred_element_type=f32)
        gate_sum = gate_sum * scale
        up_sum = up_sum * scale
        hidden = gate_sum / (1.0 + jnp.exp(-gate_sum)) * up_sum
        hidden_all[k] = jnp.where(keep, hidden, 0.0).astype(bf16)
        if k > 0:
            arrive_and_pass(k, 2)
    pass_arrive(2)
    for turn_at, k in enumerate(order):
        hidden = hidden_all[k]
        for i, target in enumerate((near, diagonal)):
            pair_out[k, i] = jnp.dot(
                hidden, down_buf[:, columns(target)], preferred_element_type=f32
            ).astype(bf16)
        pair_copy(k).start()
        for i, target in enumerate((t, across)):
            held[k, i] = jnp.dot(hidden, down_buf[:, columns(target)], preferred_element_type=f32)
        if turn_at > 0:
            pair_step(order[turn_at - 1])
        if turn_at > 1:
            cross_step(order[turn_at - 2])
    pair_step(order[-1])
    for k in order[-2:]:
        cross_step(k)
    result = resid[...] + held[0, 0]
    for k in range(1, places):
        sum_copy(k).wait_recv()
        result = result + line_in[k].astype(f32)
    out[...] = result.astype(bf16)

    @pl.when(s < places - 1)
    def _():
        for c in range(chunks):
            state_copy(c).wait_send()

    for k in range(1, places):
        for m in range(3):
            wide_sent(k, m)
        line_y(k).wait_send()
        total_copy(k).wait_send()
        sum_copy(k).wait_send()
    for m in range(3):
        pass_sent(m)
    for j in range(1, shares):
        proj_copy(j).wait_send()
        square_copy(j).wait_send()
    for k in range(places):
        for copy in (core_y, chip_y, relay_y, pair_copy, cross_copy):
            copy(k).wait_send()


def fused(units, *arrays):
    (
        stream, queries, key_matrix, value_matrix, output_gate_logits, forgetting_raw_score,
        additional_forgetting_rate, head_norm_gain, output_weight, feedforward_norm_gain,
        gate_weight, up_weight, down_weight,
    ) = arrays
    places, shares, copies = (lax.axis_size(a) for a in ("sp", "tp", "grp"))
    tokens, model_width = stream.shape
    cols = model_width // shares
    f32, bf16 = jnp.float32, jnp.bfloat16
    vmem = pl.BlockSpec(memory_space=pltpu.VMEM)
    anywhere = pl.BlockSpec(memory_space=pl.ANY)
    buffers = [
        ((model_width, units), bf16), ((model_width, units), bf16), ((units, model_width), bf16),
        (output_weight.shape, bf16), ((HK, HV), f32), ((HV // 128, HK, 128), bf16),
        ((HV // 128, HK, 128), bf16), ((places, tokens, units), bf16), ((tokens, HV), f32),
        ((shares, tokens, cols), bf16), ((shares - 1, tokens, cols), bf16), ((tokens, cols), f32),
        ((places, shares, tokens, cols), bf16), ((8, tokens), f32), ((shares - 1, 8, tokens), f32),
        ((places, 8, tokens), f32),
        ((places, 2, tokens, cols), bf16), ((places, 2, tokens, cols), bf16),
        ((places, 2, tokens, cols), f32),
        ((places, tokens, cols), bf16), ((places, tokens, cols), bf16),
        ((places, tokens, cols), bf16), ((places, tokens, cols), bf16),
    ]
    far = places - 1
    counts = [(4,)]
    for count in (
        (far, 3), (copies - 1, far, 3), (HV // 128,), (shares - 1,), (shares - 1,), (far,), (far,),
        (places,), (places,), (places,), (places,), (places,), (places,),
    ):
        counts += [count, count]
    kernel = functools.partial(fused_kernel, places, shares, copies, units)
    return pl.pallas_call(
        kernel,
        out_shape=jax.ShapeDtypeStruct((tokens, cols), bf16),
        in_specs=[vmem] * 9 + [anywhere] * 4,
        out_specs=vmem,
        scratch_shapes=[pltpu.VMEM(shape, kind) for shape, kind in buffers]
        + [pltpu.SemaphoreType.DMA(count) for count in counts],
        compiler_params=pltpu.CompilerParams(
            collective_id=0, has_side_effects=True, vmem_limit_bytes=58 * 1024 * 1024
        ),
    )(
        stream, queries, key_matrix, value_matrix, output_gate_logits, forgetting_raw_score,
        additional_forgetting_rate, head_norm_gain.reshape(1, -1), feedforward_norm_gain,
        output_weight, gate_weight, up_weight, down_weight,
    )


def spread_width(stream, queries, gate_weight):
    places, shares, copies = (lax.axis_size(a) for a in ("sp", "tp", "grp"))
    tokens, model_width = stream.shape
    depth, hidden_share = gate_weight.shape
    units = -(-hidden_share // (places * 128)) * 128
    fits = (
        shares == 4 and places > 1 and copies > 1 and queries.shape[1] == HK
        and tokens % 128 == 0 and model_width % (shares * 128) == 0 and depth % (copies * 128) == 0
        and hidden_share % 128 == 0 and places * units - hidden_share < units
        and 2 * tokens * places < 3 * hidden_share
    )
    return units if fits else 0


def local(
    stream,
    queries,
    key_matrix,
    value_matrix,
    output_gate_logits,
    forgetting_raw_score,
    additional_forgetting_rate,
    head_norm_gain,
    output_weight,
    feedforward_norm_gain,
    gate_weight,
    up_weight,
    down_weight,
):
    units = spread_width(stream, queries, gate_weight)
    if units:
        return fused(
            units, stream, queries, key_matrix, value_matrix, output_gate_logits,
            forgetting_raw_score, additional_forgetting_rate, head_norm_gain, output_weight,
            feedforward_norm_gain, gate_weight, up_weight, down_weight,
        )
    tokens = queries.shape[0]
    owned_heads = queries.shape[1] // HK
    blocks = tokens // BLOCK
    forgetting_exponent = (
        jax.nn.log_sigmoid(forgetting_raw_score) / sigmoid_sharpness + additional_forgetting_rate
    )
    query_part = split_heads(queries, blocks, owned_heads, HK) * HK ** (-0.5)
    key_part = split_heads(key_matrix, blocks, owned_heads, HK)
    value_part = split_heads(value_matrix, blocks, owned_heads, HV)
    decay_part = split_heads(forgetting_exponent, blocks, owned_heads, HK)
    within = jnp.cumsum(decay_part, axis=2)
    closing = within[:, :, -1, :]
    query_in = query_part * jnp.exp(within)
    key_in = key_part * jnp.exp(-within)
    key_end = key_part * jnp.exp(closing[:, :, None, :] - within)
    causal = jnp.tril(jnp.ones((BLOCK, BLOCK), jnp.bool_))
    scores = jnp.einsum("hntd,hnsd->hnts", query_in, key_in, precision=highest)
    scores = jnp.where(causal, scores, 0.0)
    inside = jnp.einsum("hnts,hnsv->hntv", scores, value_part, precision=highest)

    def advance(memory, inputs):
        query_block, key_block, value_block, decay_block = inputs
        final_answer = jnp.einsum("htd,hdv->htv", query_block, memory, precision=highest)
        memory = decay_block[:, :, None] * memory + jnp.einsum(
            "hsd,hsv->hdv", key_block, value_block, precision=highest
        )
        return (memory, final_answer)

    sequence = (
        jnp.moveaxis(query_in, 1, 0),
        jnp.moveaxis(key_end, 1, 0),
        jnp.moveaxis(value_part, 1, 0),
        jnp.moveaxis(jnp.exp(closing), 1, 0),
    )
    start_memory = jnp.zeros((owned_heads, HK, HV), jnp.float32)
    final_memory, earlier_blocks = lax.scan(advance, start_memory, sequence)
    device_decay = jnp.exp(jnp.sum(closing, axis=1))
    neutral = (jnp.ones_like(device_decay), jnp.zeros_like(final_memory))
    _, carried = carried_in((device_decay, final_memory), "sp", combine, neutral)
    before = jnp.cumsum(closing, axis=1) - closing
    query_far = query_in * jnp.exp(before[:, :, None, :])
    outside = jnp.einsum("hntd,hdv->hntv", query_far, carried, precision=highest)
    mixed_heads = inside + jnp.moveaxis(earlier_blocks, 0, 1) + outside
    mixed_heads = mixed_heads.transpose(1, 2, 0, 3).reshape(tokens, owned_heads, HV)
    mixed_heads = mixed_heads * lax.rsqrt(
        jnp.mean(mixed_heads * mixed_heads, axis=-1, keepdims=True) + epsilon
    )
    gated_rows = (
        mixed_heads.reshape(tokens, owned_heads * HV)
        * head_norm_gain
        * jax.nn.silu(output_gate_logits.astype(jnp.float32))
    ).astype(jnp.bfloat16)
    partial_out = jnp.dot(gated_rows, output_weight, preferred_element_type=jnp.float32)
    model_width = stream.shape[1]
    column_share = model_width // lax.axis_size("tp")
    column_start = lax.axis_index("tp") * column_share
    attn_cols = lax.psum_scatter(
        partial_out.astype(jnp.bfloat16), "tp", scatter_dimension=1, tiled=True
    ).astype(jnp.float32)
    resid_part = (
        lax.dynamic_slice_in_dim(stream, column_start, column_share, 1).astype(jnp.float32)
        + attn_cols
    )
    elementwise_power = lax.psum(jnp.sum(resid_part * resid_part, axis=1), "tp")
    gain_part = lax.dynamic_slice_in_dim(
        feedforward_norm_gain, column_start, column_share, 0
    ).astype(jnp.float32)
    rescaled_portion = (
        resid_part * lax.rsqrt(elementwise_power / model_width + epsilon)[:, None] * gain_part
    ).astype(jnp.bfloat16)
    normed = lax.all_gather(rescaled_portion, "tp", axis=1, tiled=True)
    gate_sum = jnp.dot(
        normed,
        lax.all_gather(gate_weight, "sp", axis=0, tiled=True),
        preferred_element_type=jnp.float32,
    )
    up_sum = jnp.dot(
        normed,
        lax.all_gather(up_weight, "sp", axis=0, tiled=True),
        preferred_element_type=jnp.float32,
    )
    hidden = (jax.nn.silu(gate_sum) * up_sum).astype(jnp.bfloat16)
    down_sum = jnp.dot(
        hidden,
        lax.all_gather(down_weight, "sp", axis=1, tiled=True),
        preferred_element_type=jnp.float32,
    )
    ffn_part = lax.psum_scatter(
        down_sum.astype(jnp.bfloat16), "tp", scatter_dimension=1, tiled=True
    ).astype(jnp.float32)
    return (resid_part + ffn_part).astype(jnp.bfloat16)


def solution(mesh):
    return jax.shard_map(
        local,
        mesh=mesh,
        in_specs=(
            P(("grp", "sp"), None),
            P(("grp", "sp"), "tp"),
            P(("grp", "sp"), "tp"),
            P(("grp", "sp"), "tp"),
            P(("grp", "sp"), "tp"),
            P(("grp", "sp"), "tp"),
            P(("grp", "sp"), "tp"),
            P("tp"),
            P("tp", None),
            P(),
            P("sp", "tp"),
            P("sp", "tp"),
            P("tp", "sp"),
        ),
        out_specs=P(("grp", "sp"), "tp"),
        check_vma=False,
    )
```
